512 devices in a mesh: grp: 2 (over y), fs: 32 (over z), tp: 8 (over x, core).
Axes of the slice: x: 4, y: 2, z: 32, core: 2. Of those that a mesh axis runs over, the one named last changes fastest.
The devices are a block of a 4x8x32 slice.
Arguments:
- tokens: bfloat16 [8192, 2048], P(('grp', 'fs')), parts along dimension 0, may hold values from -6 to 6
- pre_attention_gain: float32 [2048], replicated, may hold values from 0.1 to 1.9
- query_weight: bfloat16 [2048, 512], P('fs', 'tp'), may hold values from -0.125 to 0.125
- key_weight: bfloat16 [2048, 512], P('fs', 'tp'), may hold values from -0.125 to 0.125
- value_weight: bfloat16 [2048, 1024], P('fs', 'tp'), may hold values from -0.125 to 0.125
- output_gate_weight: bfloat16 [2048, 1024], P('fs', 'tp'), may hold values from -0.125 to 0.125
- decay_weight: bfloat16 [2048, 512], P('fs', 'tp'), may hold values from -0.25 to 0.25
- decay_logit_bias: float32 [512], P('tp'), may hold values from -1 to 4
- extra_log_decay: float32 [8192, 512], P(('grp', 'fs'), 'tp'), parts along dimension 0, may hold values from -0.7 to 0
- head_norm_gain: float32 [1024], P('tp'), may hold values from 0.1 to 1.9
- attention_out_weight: bfloat16 [1024, 2048], P('tp', 'fs'), may hold values from -0.1875 to 0.1875
- post_attention_gain: float32 [2048], replicated, may hold values from 0.1 to 1.9
- pre_feedforward_gain: float32 [2048], replicated, may hold values from 0.1 to 1.9
- post_feedforward_gain: float32 [2048], replicated, may hold values from 0.1 to 1.9
- up_weight: bfloat16 [2048, 8192], P('fs', 'tp'), may hold values from -0.125 to 0.125
- down_weight: bfloat16 [8192, 2048], P('tp', 'fs'), may hold values from -0.0625 to 0.0625
Outputs:
- layer_out: bfloat16 [8192, 2048], P(('grp', 'fs')), parts along dimension 0
The draws below stay inside these ranges and needn't reach their ends.
There are 2 independent parts, one for each index of `grp`. The reference program is written for one: setup_inputs(seed, part) draws one part's arguments, and reference() takes and returns one part's arrays. A program takes and returns all parts, laid end to end along the dimension named above; an argument that names none is the same for every part. Nothing has to cross between parts.
All inputs are finite; a program needn't handle non-finite values.
Results may differ from the reference program's by a relative error of at most 0.035.
Values may be sent and summed in bfloat16 or wider, within the bound.
No kernel may reach another device: no remote copies, remote signals or barrier semaphores. Data moves between devices by JAX's collectives and lax.ppermute only.
A program may use at most 64 MiB of HBM per device.

```python
import jax
import jax.numpy as jnp
from jax import lax

D = 2048
HEADS = 8
DK = 64
DV = 128
BLOCK = 64
TOK_DEV = 128
QK = 512
V = 1024
FF = 8192
TOKENS = 4096
N_TP = 8


def draw_extra_log_decay(key, part):
    first, second = jax.random.split(jax.random.fold_in(key, 11))
    chance = jax.random.uniform(first, (TOKENS, 1), jnp.float32)
    depth = jax.random.uniform(second, (TOKENS, QK), jnp.float32, minval=-0.7, maxval=-0.22)
    return jnp.where(chance < 3.0 / TOK_DEV, depth, 0.0).astype(jnp.float32)


def level_of(stream_key, extent, cuts, smallest, high):
    factor_of, own = 1.0, jax.random.fold_in(stream_key, 6)
    for axis_at, parts in cuts:
        heights = jnp.exp(jax.random.uniform(jax.random.fold_in(own, axis_at), (parts,), jnp.float32, smallest / len(cuts), high / len(cuts)))
        factor_of = factor_of * jnp.repeat(heights, extent[axis_at] // parts).reshape([-1 if axis == axis_at else 1 for axis in range(len(extent))])
    return factor_of


def scatter_about(own_key, shape, scale, limit, cuts=(), held_as=jnp.bfloat16):
    values = jax.random.normal(own_key, shape, jnp.float32) * scale
    if len(cuts) > 0:
        values = level_of(own_key, shape, cuts, -0.22, 0.18) * values
    return jnp.clip(values, min=-limit, max=limit).astype(held_as)


def setup_inputs(seed: int = 0, part: int = 0) -> dict:
    keys = jax.random.split(jax.random.key(seed), 17)
    own_keys = jax.random.split(jax.random.fold_in(keys[16], part), 17)
    return {
        "tokens": scatter_about(own_keys[0], (TOKENS, D), 1.0, 6.0, ((0, 32),)),
        "pre_attention_gain": jnp.clip(1.0 + 0.18 * jax.random.normal(keys[1], (D,), jnp.float32), 0.1, 1.9),
        "query_weight": scatter_about(keys[2], (D, QK), D ** -0.5, 0.125, ((0, 32), (1, 8))),
        "key_weight": scatter_about(keys[3], (D, QK), D ** -0.5, 0.125, ((0, 32), (1, 8))),
        "value_weight": scatter_about(keys[4], (D, V), D ** -0.5, 0.125, ((0, 32), (1, 8))),
        "output_gate_weight": scatter_about(keys[5], (D, V), D ** -0.5, 0.125, ((0, 32), (1, 8))),
        "decay_weight": scatter_about(keys[6], (D, QK), (D // 4) ** -0.5, 0.25, ((0, 32), (1, 8))),
        "decay_logit_bias": jnp.clip(-1.0 + 5.0 * jax.random.uniform(keys[7], (QK,), jnp.float32) ** level_of(keys[7], (QK,), ((0, 8),), -0.2, 0.2), -1.0, 4.0),
        "extra_log_decay": draw_extra_log_decay(jax.random.fold_in(jax.random.fold_in(keys[16], part), 71), part),
        "head_norm_gain": jnp.clip(1.0 + 0.18 * jax.random.normal(keys[9], (V,), jnp.float32), 0.1, 1.9),
        "attention_out_weight": scatter_about(keys[10], (V, D), V ** -0.5, 0.1875, ((0, 8), (1, 32))),
        "post_attention_gain": jnp.clip(1.0 + 0.18 * jax.random.normal(keys[11], (D,), jnp.float32), 0.1, 1.9),
        "pre_feedforward_gain": jnp.clip(1.0 + 0.18 * jax.random.normal(keys[12], (D,), jnp.float32), 0.1, 1.9),
        "post_feedforward_gain": jnp.clip(1.0 + 0.18 * jax.random.normal(keys[13], (D,), jnp.float32), 0.1, 1.9),
        "up_weight": scatter_about(keys[14], (D, FF), D ** -0.5, 0.125, ((0, 32), (1, 8))),
        "down_weight": scatter_about(keys[15], (FF, D), FF ** -0.5, 0.0625, ((0, 8), (1, 32))),
    }


EPS = 1e-06
GATE_NORM_SCALE = 16.0
HIGH = lax.Precision.HIGHEST

def root_norm(rows, gain):
    values = rows.astype(jnp.float32)
    return values * lax.rsqrt(lax.optimization_barrier(jnp.mean(values * values, axis=-1, keepdims=True)) + EPS) * gain

def decayed_attention(queries, keys_in, values_in, decay_log_rate):
    length, heads, key_dim = queries.shape
    value_dim = values_in.shape[-1]
    blocks = length // BLOCK

    def to_blocks(array):
        return array.reshape(blocks, BLOCK, heads, array.shape[-1]).transpose(0, 2, 1, 3)
    query_blocks = to_blocks(queries)
    key_blocks = to_blocks(keys_in)
    value_blocks = to_blocks(values_in)
    cumulative = jnp.cumsum(to_blocks(decay_log_rate), axis=2)
    causal = jnp.tril(jnp.ones((BLOCK, BLOCK), dtype=bool))[:, :, None]

    def advance(state, inputs):
        query_blk, key_blk, value_blk, cum_blk = inputs
        relative = cum_blk[:, :, None, :] - cum_blk[:, None, :, :]
        weights = jnp.exp(jnp.where(causal, relative, -jnp.inf))
        scores = jnp.einsum('hid,hjd,hijd->hij', query_blk, key_blk, weights, precision=HIGH)
        inner = jnp.einsum('hij,hjv->hiv', scores, value_blk, precision=HIGH)
        inner = inner + jnp.einsum('hid,hdv->hiv', query_blk * jnp.exp(cum_blk), state, precision=HIGH)
        last = cum_blk[:, -1:, :]
        state = state * jnp.exp(last)[:, 0, :, None] + jnp.einsum('hjd,hjv->hdv', key_blk * jnp.exp(last - cum_blk), value_blk, precision=HIGH)
        return (state, inner)
    initial = jnp.zeros((heads, key_dim, value_dim), jnp.float32)
    _, result = lax.scan(advance, initial, (query_blocks, key_blocks, value_blocks, cumulative))
    return result.transpose(0, 2, 1, 3).reshape(length, heads, value_dim)

def grouped_sum(left, right, groups):
    width = left.shape[1] // groups

    def add_group(index, total):
        start = (index * width).astype(jnp.int32)
        cols = lax.dynamic_slice_in_dim(left, start, width, 1)
        rows = lax.dynamic_slice_in_dim(right, start, width, 0)
        part = jnp.dot(cols, rows, preferred_element_type=jnp.float32)
        rounded = lax.optimization_barrier(part.astype(jnp.bfloat16))
        return total + rounded.astype(jnp.float32)
    empty = jnp.zeros((left.shape[0], right.shape[1]), jnp.float32)
    return lax.fori_loop(jnp.int32(0), jnp.int32(groups), add_group, empty)

def reference(tokens, pre_attention_gain, query_weight, key_weight, value_weight, output_gate_weight, decay_weight, decay_logit_bias, extra_log_decay, head_norm_gain, attention_out_weight, post_attention_gain, pre_feedforward_gain, post_feedforward_gain, up_weight, down_weight):
    stream_in = tokens.astype(jnp.float32)
    normed = root_norm(stream_in, pre_attention_gain).astype(jnp.bfloat16)
    query_rows = jnp.dot(normed, query_weight, preferred_element_type=jnp.float32).astype(jnp.bfloat16)
    key_rows = jnp.dot(normed, key_weight, preferred_element_type=jnp.float32).astype(jnp.bfloat16)
    value_rows = jnp.dot(normed, value_weight, preferred_element_type=jnp.float32).astype(jnp.bfloat16)
    gate_rows = jnp.dot(normed, output_gate_weight, preferred_element_type=jnp.float32).astype(jnp.bfloat16)
    decay_logits = jnp.dot(normed, decay_weight, preferred_element_type=jnp.float32)
    decay_log_rate = jax.nn.log_sigmoid(decay_logits + decay_logit_bias) / GATE_NORM_SCALE + extra_log_decay
    seqs = TOKENS // TOK_DEV
    queries = (query_rows.astype(jnp.float32) * DK ** (-0.5)).reshape(seqs, TOK_DEV, HEADS, DK)
    keys_in = key_rows.astype(jnp.float32).reshape(seqs, TOK_DEV, HEADS, DK)
    values_in = value_rows.astype(jnp.float32).reshape(seqs, TOK_DEV, HEADS, DV)
    decays = decay_log_rate.reshape(seqs, TOK_DEV, HEADS, DK)
    attended = lax.map(lambda item: decayed_attention(*item), (queries, keys_in, values_in, decays))
    attended = attended.reshape(TOKENS, HEADS, DV)
    scaled = attended * lax.rsqrt(lax.optimization_barrier(jnp.mean(attended * attended, axis=-1, keepdims=True)) + EPS)
    scaled = scaled.reshape(TOKENS, V) * head_norm_gain
    headout = (scaled * jax.nn.silu(gate_rows.astype(jnp.float32))).astype(jnp.bfloat16)
    mixed = grouped_sum(headout, attention_out_weight, N_TP)
    stream = stream_in + root_norm(mixed, post_attention_gain)
    normed_mid = root_norm(stream, pre_feedforward_gain).astype(jnp.bfloat16)
    hidden = jnp.square(jax.nn.relu(jnp.dot(normed_mid, up_weight, preferred_element_type=jnp.float32))).astype(jnp.bfloat16)
    feedfwd = grouped_sum(hidden, down_weight, N_TP)
    return (stream + root_norm(feedfwd, post_feedforward_gain)).astype(jnp.bfloat16)
```

```python
import functools

import jax
import jax.numpy as jnp
from jax import lax
from jax.experimental import pallas as pl
from jax.experimental.pallas import tpu as pltpu
from jax.sharding import PartitionSpec as P

DK = 64
DV = 128
SUB = 8
FF_CHUNK = 256

EPS = 1e-06
GATE_NORM_SCALE = 16.0
HIGH = lax.Precision.HIGHEST
F32 = jnp.float32
BF16 = jnp.bfloat16


def root_norm(rows, gain):
    return rows * lax.rsqrt(jnp.mean(rows * rows, axis=-1, keepdims=True) + EPS) * gain


def attend_body(acc_ref, bias_ref, extra_ref, gain_ref, out_ref):
    length = acc_ref.shape[0]
    subs = length // SUB
    rounded = lambda lo, hi: acc_ref[:, lo:hi].astype(BF16).astype(F32)
    v = rounded(0, DV)
    g = rounded(DV, 2 * DV)
    q = rounded(2 * DV, 2 * DV + DK) * DK ** (-0.5)
    k = rounded(2 * DV + DK, 2 * DV + 2 * DK)
    pre = acc_ref[:, 2 * DV + 2 * DK : 2 * DV + 3 * DK] + bias_ref[...]
    log_sig = jnp.minimum(pre, 0.0) - jnp.log1p(jnp.exp(-jnp.abs(pre)))
    log_decay = log_sig / GATE_NORM_SCALE + extra_ref[...]
    row = lax.broadcasted_iota(jnp.int32, (length, length), 0)
    col = lax.broadcasted_iota(jnp.int32, (length, length), 1)
    dot = functools.partial(lax.dot_general, precision=HIGH, preferred_element_type=F32)
    nn, nt = (((1,), (0,)), ((), ())), (((1,), (1,)), ((), ()))
    cum = dot((row >= col).astype(F32), log_decay, nn)
    cum3, q3, k3 = (a.reshape(subs, SUB, DK) for a in (cum, q, k))
    inside = []
    for j in range(SUB):
        gap = jnp.minimum(cum3 - cum3[:, j : j + 1, :], 0.0)
        inside.append(jnp.sum(q3 * k3[:, j : j + 1, :] * jnp.exp(gap), axis=-1, keepdims=True))
    near = jnp.zeros((length, length), F32)
    for j in range(SUB):
        near = jnp.where(lax.rem(col, SUB) == j, inside[j].reshape(length, 1), near)
    same = (row // SUB == col // SUB) & (row >= col)
    far = [jnp.zeros((SUB, length), F32)]
    for i in range(1, subs):
        at = i * SUB
        mark = cum[at - 1 : at, :]
        left = q[at : at + SUB, :] * jnp.exp(jnp.minimum(cum[at : at + SUB, :] - mark, 0.0))
        right = k * jnp.exp(jnp.minimum(mark - cum, 0.0))
        far.append(dot(left, right, nt))
    scores = jnp.where(same, near, jnp.where(row // SUB > col // SUB, jnp.concatenate(far, 0), 0.0))
    attended = dot(scores, v, nn)
    scaled = attended * lax.rsqrt(jnp.mean(attended * attended, axis=-1, keepdims=True) + EPS)
    out_ref[...] = (scaled * gain_ref[...] * (g / (1.0 + jnp.exp(-g)))).astype(out_ref.dtype)


def attend(acc, bias, extra, gain):
    length = acc.shape[0]
    return pl.pallas_call(
        attend_body,
        out_shape=jax.ShapeDtypeStruct((length, DV), BF16),
        compiler_params=pltpu.CompilerParams(vmem_limit_bytes=16 * 2**20),
        cost_estimate=pl.CostEstimate(flops=40_000_000, bytes_accessed=500_000, transcendentals=400_000),
        name="attend",
    )(acc, bias, extra, gain)


def feed_body(rows_ref, up_ref, down_ref, out_ref, sum_ref):
    step = pl.program_id(0)
    act = jnp.dot(rows_ref[...], up_ref[...], preferred_element_type=F32)
    act = jnp.square(jnp.maximum(act, 0.0)).astype(BF16)
    part = lax.dot_general(act, down_ref[...], (((1,), (1,)), ((), ())), preferred_element_type=F32)

    @pl.when(step == 0)
    def _():
        sum_ref[...] = part

    @pl.when(step > 0)
    def _():
        sum_ref[...] += part

    @pl.when(step == pl.num_programs(0) - 1)
    def _():
        out_ref[...] = sum_ref[...].astype(out_ref.dtype)


def feed(rows, both):
    length, width = rows.shape
    units = both.shape[1] // 2
    steps = units // FF_CHUNK
    return pl.pallas_call(
        feed_body,
        grid=(steps,),
        in_specs=[
            pl.BlockSpec((length, width), lambda s: (0, 0)),
            pl.BlockSpec((width, FF_CHUNK), lambda s: (0, s)),
            pl.BlockSpec((width, FF_CHUNK), lambda s: (0, s + steps)),
        ],
        out_specs=pl.BlockSpec((length, width), lambda s: (0, 0)),
        out_shape=jax.ShapeDtypeStruct((length, width), BF16),
        scratch_shapes=[pltpu.VMEM((length, width), F32)],
        compiler_params=pltpu.CompilerParams(
            dimension_semantics=("arbitrary",), vmem_limit_bytes=58 * 2**20
        ),
        cost_estimate=pl.CostEstimate(
            flops=4 * length * width * units, bytes_accessed=4 * width * units, transcendentals=0
        ),
        name="feed",
    )(rows, both, both)


def share_of_sum(part, axis):
    peers = lax.axis_size(axis)
    blocks = part.reshape(peers, part.shape[0] // peers, part.shape[1])
    arrived = lax.all_to_all(blocks, axis, split_axis=0, concat_axis=0, tiled=True)
    return arrived.astype(F32).sum(axis=0)


def local(
    tokens,
    pre_attention_gain,
    query_weight,
    key_weight,
    value_weight,
    output_gate_weight,
    decay_weight,
    decay_logit_bias,
    extra_log_decay,
    head_norm_gain,
    attention_out_weight,
    post_attention_gain,
    pre_feedforward_gain,
    post_feedforward_gain,
    up_weight,
    down_weight,
):
    groups, fs = lax.axis_size("grp"), lax.axis_size("fs")
    both = lax.all_gather(
        jnp.concatenate([up_weight, down_weight.T], 1), "fs", axis=0, tiled=True
    )
    out_piece = attention_out_weight.T
    out_rows = lax.all_to_all(
        jnp.broadcast_to(out_piece[None], (fs, *out_piece.shape)), "fs", 0, 0, tiled=True
    ).reshape(-1, out_piece.shape[1])
    whole = jnp.concatenate(
        [value_weight, output_gate_weight, query_weight, key_weight, decay_weight], 1
    )
    half = whole.shape[1] // 2
    side = lax.rem(lax.axis_index("grp"), 2)
    mine = lax.all_gather(
        lax.dynamic_slice_in_dim(whole, side * half, half, 1), "fs", axis=0, tiled=True
    )
    theirs = lax.ppermute(mine, "grp", [(i, i ^ 1) for i in range(groups)])

    normed = root_norm(tokens.astype(F32), pre_attention_gain).astype(BF16)
    acc_mine = jnp.dot(normed, mine, preferred_element_type=F32)
    acc_theirs = jnp.dot(normed, theirs, preferred_element_type=F32)
    first = side == 0
    acc = jnp.concatenate(
        [jnp.where(first, acc_mine, acc_theirs), jnp.where(first, acc_theirs, acc_mine)], 1
    )
    headout = attend(acc, decay_logit_bias[None], extra_log_decay, head_norm_gain[None])

    mix_part = lax.dot_general(
        headout, out_rows, (((1,), (1,)), ((), ())), preferred_element_type=F32
    )
    mixed = share_of_sum(mix_part.astype(BF16), "tp")
    share = mixed.shape[0]
    own_tokens = lax.dynamic_slice_in_dim(tokens, lax.axis_index("tp") * share, share, 0)
    stream = own_tokens.astype(F32) + root_norm(mixed, post_attention_gain)
    normed_mid = root_norm(stream, pre_feedforward_gain).astype(BF16)
    rows = lax.all_gather(normed_mid, "tp", axis=0, tiled=True)
    feed_share = share_of_sum(feed(rows, both), "tp")
    out_share = (stream + root_norm(feed_share, post_feedforward_gain)).astype(BF16)
    return lax.all_gather(out_share, "tp", axis=0, tiled=True)


def solution(mesh):
    return jax.shard_map(
        local,
        mesh=mesh,
        in_specs=(
            P(("grp", "fs"), None),
            P(),
            P("fs", "tp"),
            P("fs", "tp"),
            P("fs", "tp"),
            P("fs", "tp"),
            P("fs", "tp"),
            P("tp"),
            P(("grp", "fs"), "tp"),
            P("tp"),
            P("tp", "fs"),
            P(),
            P(),
            P(),
            P("fs", "tp"),
            P("tp", "fs"),
        ),
        out_specs=P(("grp", "fs"), None),
        check_vma=False,
    )
```

```python
import functools

import jax
import jax.numpy as jnp
from jax import lax
from jax.experimental import pallas as pl
from jax.experimental.pallas import tpu as pltpu
from jax.sharding import PartitionSpec as P

DK = 64
DV = 128
SUB = 8
FF_CHUNK = 256

EPS = 1e-06
GATE_NORM_SCALE = 16.0
WEIGHT_SCALE = 2.0**16
HIGH = lax.Precision.HIGHEST
F32 = jnp.float32
BF16 = jnp.bfloat16


def root_norm(rows, gain):
    return rows * lax.rsqrt(jnp.mean(rows * rows, axis=-1, keepdims=True) + EPS) * gain


def attend_body(acc_ref, bias_ref, extra_ref, gain_ref, out_ref):
    length = acc_ref.shape[0]
    subs = length // SUB
    rounded = lambda lo, hi: acc_ref[:, lo:hi].astype(BF16).astype(F32)
    v = rounded(0, DV)
    g = rounded(DV, 2 * DV)
    q = rounded(2 * DV, 2 * DV + DK) * DK ** (-0.5)
    k = rounded(2 * DV + DK, 2 * DV + 2 * DK)
    pre = acc_ref[:, 2 * DV + 2 * DK : 2 * DV + 3 * DK] + bias_ref[...]
    log_sig = jnp.minimum(pre, 0.0) - jnp.log1p(jnp.exp(-jnp.abs(pre)))
    log_decay = log_sig / GATE_NORM_SCALE + extra_ref[...]
    row = lax.broadcasted_iota(jnp.int32, (length, length), 0)
    col = lax.broadcasted_iota(jnp.int32, (length, length), 1)
    dot = functools.partial(lax.dot_general, precision=HIGH, preferred_element_type=F32)
    nn, nt = (((1,), (0,)), ((), ())), (((1,), (1,)), ((), ()))
    cum = dot((row >= col).astype(F32), log_decay, nn)
    cum3, q3, k3 = (a.reshape(subs, SUB, DK) for a in (cum, q, k))
    inside = []
    for j in range(SUB):
        gap = jnp.minimum(cum3 - cum3[:, j : j + 1, :], 0.0)
        inside.append(jnp.sum(q3 * k3[:, j : j + 1, :] * jnp.exp(gap), axis=-1, keepdims=True))
    near = jnp.zeros((length, length), F32)
    for j in range(SUB):
        near = jnp.where(lax.rem(col, SUB) == j, inside[j].reshape(length, 1), near)
    same = (row // SUB == col // SUB) & (row >= col)
    far = [jnp.zeros((SUB, length), F32)]
    for i in range(1, subs):
        at = i * SUB
        mark = cum[at - 1 : at, :]
        left = q[at : at + SUB, :] * jnp.exp(jnp.minimum(cum[at : at + SUB, :] - mark, 0.0))
        right = k * jnp.exp(jnp.minimum(mark - cum, 0.0))
        far.append(dot(left, right, nt))
    scores = jnp.where(same, near, jnp.where(row // SUB > col // SUB, jnp.concatenate(far, 0), 0.0))
    attended = dot(scores, v, nn)
    scaled = attended * lax.rsqrt(jnp.mean(attended * attended, axis=-1, keepdims=True) + EPS)
    out_ref[...] = (scaled * gain_ref[...] * (g / (1.0 + jnp.exp(-g)))).astype(out_ref.dtype)


def attend(acc, bias, extra, gain):
    length = acc.shape[0]
    return pl.pallas_call(
        attend_body,
        out_shape=jax.ShapeDtypeStruct((length, DV), BF16),
        compiler_params=pltpu.CompilerParams(vmem_limit_bytes=16 * 2**20),
        cost_estimate=pl.CostEstimate(flops=40_000_000, bytes_accessed=500_000, transcendentals=400_000),
        name="attend",
    )(acc, bias, extra, gain)


def feed_body(rows_ref, up_ref, down_ref, out_ref, sum_ref):
    step = pl.program_id(0)
    act = jnp.dot(rows_ref[...], up_ref[...], preferred_element_type=F32)
    act = jnp.square(jnp.maximum(act, 0.0)).astype(BF16)
    part = lax.dot_general(act, down_ref[...], (((1,), (1,)), ((), ())), preferred_element_type=F32)

    @pl.when(step == 0)
    def _():
        sum_ref[...] = part

    @pl.when(step > 0)
    def _():
        sum_ref[...] += part

    @pl.when(step == pl.num_programs(0) - 1)
    def _():
        out_ref[...] = sum_ref[...].astype(out_ref.dtype)


def feed(rows, both):
    length, width = rows.shape
    units = both.shape[1] // 2
    steps = units // FF_CHUNK
    return pl.pallas_call(
        feed_body,
        grid=(steps,),
        in_specs=[
            pl.BlockSpec((length, width), lambda s: (0, 0)),
            pl.BlockSpec((width, FF_CHUNK), lambda s: (0, s)),
            pl.BlockSpec((width, FF_CHUNK), lambda s: (0, s + steps)),
        ],
        out_specs=pl.BlockSpec((length, width), lambda s: (0, 0)),
        out_shape=jax.ShapeDtypeStruct((length, width), BF16),
        scratch_shapes=[pltpu.VMEM((length, width), F32)],
        compiler_params=pltpu.CompilerParams(
            dimension_semantics=("arbitrary",), vmem_limit_bytes=58 * 2**20
        ),
        cost_estimate=pl.CostEstimate(
            flops=4 * length * width * units, bytes_accessed=4 * width * units, transcendentals=0
        ),
        name="feed",
    )(rows, both, both)


def share_of_sum(part, axis):
    peers = lax.axis_size(axis)
    blocks = part.reshape(peers, part.shape[0] // peers, part.shape[1])
    arrived = lax.all_to_all(blocks, axis, split_axis=0, concat_axis=0, tiled=True)
    return arrived.astype(F32).sum(axis=0)


def local(
    tokens,
    pre_attention_gain,
    query_weight,
    key_weight,
    value_weight,
    output_gate_weight,
    decay_weight,
    decay_logit_bias,
    extra_log_decay,
    head_norm_gain,
    attention_out_weight,
    post_attention_gain,
    pre_feedforward_gain,
    post_feedforward_gain,
    up_weight,
    down_weight,
):
    both = lax.all_gather(
        jnp.concatenate([up_weight, down_weight.T], 1), "fs", axis=0, tiled=True
    )
    pieces = (value_weight, output_gate_weight, query_weight, key_weight, decay_weight)
    whole = jnp.concatenate([*pieces, attention_out_weight.T], 1)
    sent = (whole.astype(F32) * WEIGHT_SCALE).astype(jnp.float16)
    held = lax.all_gather(sent, "fs", axis=0, tiled=True)
    width = sum(p.shape[1] for p in pieces)
    unscaled = lambda w: (w.astype(F32) * (1.0 / WEIGHT_SCALE)).astype(BF16)
    out_rows = unscaled(held[:, width:])
    normed = root_norm(tokens.astype(F32), pre_attention_gain).astype(BF16)
    acc = jnp.dot(normed, unscaled(held[:, :width]), preferred_element_type=F32)
    headout = attend(acc, decay_logit_bias[None], extra_log_decay, head_norm_gain[None])

    mix_part = lax.dot_general(
        headout, out_rows, (((1,), (1,)), ((), ())), preferred_element_type=F32
    )
    mixed = share_of_sum(mix_part.astype(BF16), "tp")
    share = mixed.shape[0]
    own_tokens = lax.dynamic_slice_in_dim(tokens, lax.axis_index("tp") * share, share, 0)
    stream = own_tokens.astype(F32) + root_norm(mixed, post_attention_gain)
    normed_mid = root_norm(stream, pre_feedforward_gain).astype(BF16)
    rows = lax.all_gather(normed_mid, "tp", axis=0, tiled=True)
    feed_share = share_of_sum(feed(rows, both), "tp")
    out_share = (stream + root_norm(feed_share, post_feedforward_gain)).astype(BF16)
    return lax.all_gather(out_share, "tp", axis=0, tiled=True)


def solution(mesh):
    return jax.shard_map(
        local,
        mesh=mesh,
        in_specs=(
            P(("grp", "fs"), None),
            P(),
            P("fs", "tp"),
            P("fs", "tp"),
            P("fs", "tp"),
            P("fs", "tp"),
            P("fs", "tp"),
            P("tp"),
            P(("grp", "fs"), "tp"),
            P("tp"),
            P("tp", "fs"),
            P(),
            P(),
            P(),
            P("fs", "tp"),
            P("tp", "fs"),
        ),
        out_specs=P(("grp", "fs"), None),
        check_vma=False,
    )
```

```python
import functools

import jax
import jax.numpy as jnp
from jax import lax
from jax.experimental import pallas as pl
from jax.experimental.pallas import tpu as pltpu
from jax.sharding import PartitionSpec as P

DK = 64
DV = 128
SUB = 8
FF_CHUNK = 512

EPS = 1e-06
GATE_NORM_SCALE = 16.0
WEIGHT_SCALE = 2.0**16
HIGH = lax.Precision.HIGHEST
F32 = jnp.float32
BF16 = jnp.bfloat16


def root_norm(rows, gain):
    return rows * lax.rsqrt(jnp.mean(rows * rows, axis=-1, keepdims=True) + EPS) * gain


def attend_body(acc_ref, bias_ref, extra_ref, gain_ref, out_ref):
    length = acc_ref.shape[0]
    subs = length // SUB
    rounded = lambda lo, hi: acc_ref[:, lo:hi].astype(BF16).astype(F32)
    v = rounded(0, DV)
    g = rounded(DV, 2 * DV)
    q = rounded(2 * DV, 2 * DV + DK) * DK ** (-0.5)
    k = rounded(2 * DV + DK, 2 * DV + 2 * DK)
    pre = acc_ref[:, 2 * DV + 2 * DK : 2 * DV + 3 * DK] + bias_ref[...]
    log_sig = jnp.minimum(pre, 0.0) - jnp.log1p(jnp.exp(-jnp.abs(pre)))
    log_decay = log_sig / GATE_NORM_SCALE + extra_ref[...]
    row = lax.broadcasted_iota(jnp.int32, (length, length), 0)
    col = lax.broadcasted_iota(jnp.int32, (length, length), 1)
    dot = functools.partial(lax.dot_general, precision=HIGH, preferred_element_type=F32)
    nn, nt = (((1,), (0,)), ((), ())), (((1,), (1,)), ((), ()))
    cum = dot((row >= col).astype(F32), log_decay, nn)
    cum3, q3, k3 = (a.reshape(subs, SUB, DK) for a in (cum, q, k))
    inside = []
    for j in range(SUB):
        gap = jnp.minimum(cum3 - cum3[:, j : j + 1, :], 0.0)
        inside.append(jnp.sum(q3 * k3[:, j : j + 1, :] * jnp.exp(gap), axis=-1, keepdims=True))
    near = jnp.zeros((length, length), F32)
    for j in range(SUB):
        near = jnp.where(lax.rem(col, SUB) == j, inside[j].reshape(length, 1), near)
    same = (row // SUB == col // SUB) & (row >= col)
    far = [jnp.zeros((SUB, length), F32)]
    for i in range(1, subs):
        at = i * SUB
        mark = cum[at - 1 : at, :]
        left = q[at : at + SUB, :] * jnp.exp(jnp.minimum(cum[at : at + SUB, :] - mark, 0.0))
        right = k * jnp.exp(jnp.minimum(mark - cum, 0.0))
        far.append(dot(left, right, nt))
    scores = jnp.where(same, near, jnp.where(row // SUB > col // SUB, jnp.concatenate(far, 0), 0.0))
    attended = dot(scores, v, nn)
    scaled = attended * lax.rsqrt(jnp.mean(attended * attended, axis=-1, keepdims=True) + EPS)
    out_ref[...] = (scaled * gain_ref[...] * (g / (1.0 + jnp.exp(-g)))).astype(out_ref.dtype)


def attend(acc, bias, extra, gain):
    length = acc.shape[0]
    return pl.pallas_call(
        attend_body,
        out_shape=jax.ShapeDtypeStruct((length, DV), BF16),
        compiler_params=pltpu.CompilerParams(vmem_limit_bytes=16 * 2**20),
        cost_estimate=pl.CostEstimate(flops=40_000_000, bytes_accessed=500_000, transcendentals=400_000),
        name="attend",
    )(acc, bias, extra, gain)


def feed_body(rows_ref, up_ref, down_ref, out_ref, sum_ref):
    step = pl.program_id(0)
    act = jnp.dot(rows_ref[...], up_ref[...], preferred_element_type=F32)
    act = jnp.square(jnp.maximum(act, 0.0)).astype(BF16)
    part = lax.dot_general(act, down_ref[...], (((1,), (1,)), ((), ())), preferred_element_type=F32)

    @pl.when(step == 0)
    def _():
        sum_ref[...] = part

    @pl.when(step > 0)
    def _():
        sum_ref[...] += part

    @pl.when(step == pl.num_programs(0) - 1)
    def _():
        out_ref[...] = sum_ref[...].astype(out_ref.dtype)


def feed(rows, both):
    length, width = rows.shape
    units = both.shape[1] // 2
    steps = units // FF_CHUNK
    return pl.pallas_call(
        feed_body,
        grid=(steps,),
        in_specs=[
            pl.BlockSpec((length, width), lambda s: (0, 0)),
            pl.BlockSpec((width, FF_CHUNK), lambda s: (0, s)),
            pl.BlockSpec((width, FF_CHUNK), lambda s: (0, s + steps)),
        ],
        out_specs=pl.BlockSpec((length, width), lambda s: (0, 0)),
        out_shape=jax.ShapeDtypeStruct((length, width), BF16),
        scratch_shapes=[pltpu.VMEM((length, width), F32)],
        compiler_params=pltpu.CompilerParams(
            dimension_semantics=("arbitrary",), vmem_limit_bytes=48 * 2**20
        ),
        cost_estimate=pl.CostEstimate(
            flops=4 * length * width * units, bytes_accessed=4 * width * units, transcendentals=0
        ),
        name="feed",
    )(rows, both, both)


def share_of_sum(part, axis):
    peers = lax.axis_size(axis)
    blocks = part.reshape(peers, part.shape[0] // peers, part.shape[1])
    arrived = lax.all_to_all(blocks, axis, split_axis=0, concat_axis=0, tiled=True)
    return arrived.astype(F32).sum(axis=0)


def local(
    tokens,
    pre_attention_gain,
    query_weight,
    key_weight,
    value_weight,
    output_gate_weight,
    decay_weight,
    decay_logit_bias,
    extra_log_decay,
    head_norm_gain,
    attention_out_weight,
    post_attention_gain,
    pre_feedforward_gain,
    post_feedforward_gain,
    up_weight,
    down_weight,
):
    both = lax.all_gather(
        jnp.concatenate([up_weight, down_weight.T], 1), "fs", axis=0, tiled=True
    )
    pieces = (value_weight, output_gate_weight, query_weight, key_weight, decay_weight)
    whole = jnp.concatenate([*pieces, attention_out_weight.T], 1)
    sent = (whole.astype(F32) * WEIGHT_SCALE).astype(jnp.float16)
    held = lax.all_gather(sent, "fs", axis=0, tiled=True)
    width = sum(p.shape[1] for p in pieces)
    unscaled = lambda w: (w.astype(F32) * (1.0 / WEIGHT_SCALE)).astype(BF16)
    out_rows = unscaled(held[:, width:])
    normed = root_norm(tokens.astype(F32), pre_attention_gain).astype(BF16)
    acc = jnp.dot(normed, unscaled(held[:, :width]), preferred_element_type=F32)
    headout = attend(acc, decay_logit_bias[None], extra_log_decay, head_norm_gain[None])

    mix_part = lax.dot_general(
        headout, out_rows, (((1,), (1,)), ((), ())), preferred_element_type=F32
    )
    mixed = share_of_sum(mix_part.astype(BF16), "tp")
    share = mixed.shape[0]
    own_tokens = lax.dynamic_slice_in_dim(tokens, lax.axis_index("tp") * share, share, 0)
    stream = own_tokens.astype(F32) + root_norm(mixed, post_attention_gain)
    normed_mid = root_norm(stream, pre_feedforward_gain).astype(BF16)
    rows = lax.all_gather(normed_mid, "tp", axis=0, tiled=True)
    feed_share = share_of_sum(feed(rows, both), "tp")
    out_share = (stream + root_norm(feed_share, post_feedforward_gain)).astype(BF16)
    return lax.all_gather(out_share, "tp", axis=0, tiled=True)


def solution(mesh):
    return jax.shard_map(
        local,
        mesh=mesh,
        in_specs=(
            P(("grp", "fs"), None),
            P(),
            P("fs", "tp"),
            P("fs", "tp"),
            P("fs", "tp"),
            P("fs", "tp"),
            P("fs", "tp"),
            P("tp"),
            P(("grp", "fs"), "tp"),
            P("tp"),
            P("tp", "fs"),
            P(),
            P(),
            P(),
            P("fs", "tp"),
            P("tp", "fs"),
        ),
        out_specs=P(("grp", "fs"), None),
        check_vma=False,
    )
```

```python
import functools

import jax
import jax.numpy as jnp
from jax import lax
from jax.experimental import pallas as pl
from jax.experimental.pallas import tpu as pltpu
from jax.sharding import PartitionSpec as P

DK = 64
DV = 128
SUB = 8

EPS = 1e-06
GATE_NORM_SCALE = 16.0
WEIGHT_SCALE = 2.0**16
HIGH = lax.Precision.HIGHEST
F32 = jnp.float32
BF16 = jnp.bfloat16


def root_norm(rows, gain):
    return rows * lax.rsqrt(jnp.mean(rows * rows, axis=-1, keepdims=True) + EPS) * gain


def attend_body(acc_ref, bias_ref, extra_ref, gain_ref, out_ref):
    length = acc_ref.shape[0]
    subs = length // SUB
    rounded = lambda lo, hi: acc_ref[:, lo:hi].astype(BF16).astype(F32)
    v = rounded(0, DV)
    g = rounded(DV, 2 * DV)
    q = rounded(2 * DV, 2 * DV + DK) * DK ** (-0.5)
    k = rounded(2 * DV + DK, 2 * DV + 2 * DK)
    pre = acc_ref[:, 2 * DV + 2 * DK : 2 * DV + 3 * DK] + bias_ref[...]
    log_sig = jnp.minimum(pre, 0.0) - jnp.log1p(jnp.exp(-jnp.abs(pre)))
    log_decay = log_sig / GATE_NORM_SCALE + extra_ref[...]
    row = lax.broadcasted_iota(jnp.int32, (length, length), 0)
    col = lax.broadcasted_iota(jnp.int32, (length, length), 1)
    dot = functools.partial(lax.dot_general, precision=HIGH, preferred_element_type=F32)
    nn, nt = (((1,), (0,)), ((), ())), (((1,), (1,)), ((), ()))
    cum = dot((row >= col).astype(F32), log_decay, nn)
    cum3, q3, k3 = (a.reshape(subs, SUB, DK) for a in (cum, q, k))
    inside = []
    for j in range(SUB):
        gap = jnp.minimum(cum3 - cum3[:, j : j + 1, :], 0.0)
        inside.append(jnp.sum(q3 * k3[:, j : j + 1, :] * jnp.exp(gap), axis=-1, keepdims=True))
    near = jnp.zeros((length, length), F32)
    for j in range(SUB):
        near = jnp.where(lax.rem(col, SUB) == j, inside[j].reshape(length, 1), near)
    same = (row // SUB == col // SUB) & (row >= col)
    far = [jnp.zeros((SUB, length), F32)]
    for i in range(1, subs):
        at = i * SUB
        mark = cum[at - 1 : at, :]
        left = q[at : at + SUB, :] * jnp.exp(jnp.minimum(cum[at : at + SUB, :] - mark, 0.0))
        right = k * jnp.exp(jnp.minimum(mark - cum, 0.0))
        far.append(dot(left, right, nt))
    scores = jnp.where(same, near, jnp.where(row // SUB > col // SUB, jnp.concatenate(far, 0), 0.0))
    attended = dot(scores, v, nn)
    scaled = attended * lax.rsqrt(jnp.mean(attended * attended, axis=-1, keepdims=True) + EPS)
    out_ref[...] = (scaled * gain_ref[...] * (g / (1.0 + jnp.exp(-g)))).astype(out_ref.dtype)


def attend(acc, bias, extra, gain):
    length = acc.shape[0]
    return pl.pallas_call(
        attend_body,
        out_shape=jax.ShapeDtypeStruct((length, DV), BF16),
        compiler_params=pltpu.CompilerParams(vmem_limit_bytes=16 * 2**20),
        cost_estimate=pl.CostEstimate(flops=40_000_000, bytes_accessed=500_000, transcendentals=400_000),
        name="attend",
    )(acc, bias, extra, gain)


def feed_body(halves, rows_ref, weight_ref, part_ref, out_ref, sum_ref, act_ref):
    step = pl.program_id(0)

    @pl.when(step < halves)
    def _():
        product = jnp.dot(rows_ref[...], weight_ref[...], preferred_element_type=F32)

        @pl.when(step == 0)
        def _():
            sum_ref[...] = product

        @pl.when(step > 0)
        def _():
            sum_ref[...] += product

        @pl.when(step == halves - 1)
        def _():
            act_ref[...] = jnp.square(jnp.maximum(sum_ref[...], 0.0)).astype(BF16)

    @pl.when(step >= halves)
    def _():
        product = lax.dot_general(
            act_ref[...], weight_ref[...], (((1,), (1,)), ((), ())), preferred_element_type=F32
        )
        out_ref[...] = (product + part_ref[...]).astype(out_ref.dtype)


def feed(rows, both, part):
    length, width = rows.shape
    units = both.shape[1] // 2
    halves = 2
    block = width // halves
    later = lambda s: (0, jnp.maximum(s - halves, 0))
    return pl.pallas_call(
        functools.partial(feed_body, halves),
        grid=(2 * halves,),
        in_specs=[
            pl.BlockSpec((length, block), lambda s: (0, jnp.minimum(s, halves - 1))),
            pl.BlockSpec((block, units), lambda s: (lax.rem(s, halves), s // halves)),
            pl.BlockSpec((length, block), later),
        ],
        out_specs=pl.BlockSpec((length, block), later),
        out_shape=jax.ShapeDtypeStruct((length, width), BF16),
        scratch_shapes=[pltpu.VMEM((length, units), F32), pltpu.VMEM((length, units), BF16)],
        compiler_params=pltpu.CompilerParams(
            dimension_semantics=("arbitrary",), vmem_limit_bytes=48 * 2**20
        ),
        cost_estimate=pl.CostEstimate(
            flops=4 * length * width * units, bytes_accessed=4 * width * units, transcendentals=0
        ),
        name="feed",
    )(rows, both, part)


def pack_body(first, up_ref, down_ref, out_ref, held, arrived, left):
    width = up_ref.shape[1] - first
    brought = []
    for i, source in enumerate((up_ref, down_ref)):
        copy = pltpu.make_async_copy(source.at[:, pl.ds(first, width)], held.at[i], arrived.at[i])
        copy.start()
        brought.append(copy)
    sent = []
    for i, copy in enumerate(brought):
        copy.wait()
        out = pltpu.make_async_copy(held.at[i], out_ref.at[:, pl.ds(i * width, width)], left.at[i])
        out.start()
        sent.append(out)
    for out in sent:
        out.wait()


def pack(up, down, first):
    depth, width = up.shape[0], up.shape[1] - first
    return pl.pallas_call(
        functools.partial(pack_body, first),
        in_specs=[pl.BlockSpec(memory_space=pltpu.HBM)] * 2,
        out_specs=pl.BlockSpec(memory_space=pltpu.HBM),
        out_shape=jax.ShapeDtypeStruct((depth, 2 * width), up.dtype),
        scratch_shapes=[
            pltpu.VMEM((2, depth, width), up.dtype),
            pltpu.SemaphoreType.DMA((2,)),
            pltpu.SemaphoreType.DMA((2,)),
        ],
        compiler_params=pltpu.CompilerParams(vmem_limit_bytes=62 * 2**20),
        name="pack",
    )(up, down)


def share_of_sum(part, axis):
    peers = lax.axis_size(axis)
    blocks = part.reshape(peers, part.shape[0] // peers, part.shape[1])
    arrived = lax.all_to_all(blocks, axis, split_axis=0, concat_axis=0, tiled=True)
    return arrived.astype(F32).sum(axis=0)


def local(
    tokens,
    pre_attention_gain,
    query_weight,
    key_weight,
    value_weight,
    output_gate_weight,
    decay_weight,
    decay_logit_bias,
    extra_log_decay,
    head_norm_gain,
    attention_out_weight,
    post_attention_gain,
    pre_feedforward_gain,
    post_feedforward_gain,
    up_weight,
    down_weight,
):
    apart = up_weight.shape[1] // 8
    down_rows = down_weight.T
    both = lax.all_gather(pack(up_weight, down_rows, apart), "fs", axis=0, tiled=True)
    pieces = (value_weight, output_gate_weight, query_weight, key_weight, decay_weight)
    pieces += (attention_out_weight.T, up_weight[:, :apart], down_rows[:, :apart])
    sent = (jnp.concatenate(pieces, 1).astype(F32) * WEIGHT_SCALE).astype(jnp.float16)
    held = lax.all_gather(sent, "fs", axis=0, tiled=True)
    tokens, held = lax.optimization_barrier((tokens, held))
    unscaled = lambda w: (w.astype(F32) * (1.0 / WEIGHT_SCALE)).astype(BF16)
    ends = [sum(p.shape[1] for p in pieces[:i]) for i in (5, 6, 7, 8)]
    projections = unscaled(held[:, : ends[0]])
    out_rows, up_apart, down_apart = (
        unscaled(held[:, lo:hi]) for lo, hi in zip(ends[:-1], ends[1:])
    )
    normed = root_norm(tokens.astype(F32), pre_attention_gain).astype(BF16)
    acc = jnp.dot(normed, projections, preferred_element_type=F32)
    headout = attend(acc, decay_logit_bias[None], extra_log_decay, head_norm_gain[None])

    mix_part = lax.dot_general(
        headout, out_rows, (((1,), (1,)), ((), ())), preferred_element_type=F32
    )
    mixed = share_of_sum(mix_part.astype(BF16), "tp")
    share = mixed.shape[0]
    own_tokens = lax.dynamic_slice_in_dim(tokens, lax.axis_index("tp") * share, share, 0)
    stream = own_tokens.astype(F32) + root_norm(mixed, post_attention_gain)
    normed_mid = root_norm(stream, pre_feedforward_gain).astype(BF16)
    rows = lax.all_gather(normed_mid, "tp", axis=0, tiled=True)
    act = jnp.square(jax.nn.relu(jnp.dot(rows, up_apart, preferred_element_type=F32))).astype(BF16)
    part = lax.dot_general(act, down_apart, (((1,), (1,)), ((), ())), preferred_element_type=F32)
    feed_share = share_of_sum(feed(rows, both, part), "tp")
    out_share = (stream + root_norm(feed_share, post_feedforward_gain)).astype(BF16)
    return lax.all_gather(out_share, "tp", axis=0, tiled=True)


def solution(mesh):
    return jax.shard_map(
        local,
        mesh=mesh,
        in_specs=(
            P(("grp", "fs"), None),
            P(),
            P("fs", "tp"),
            P("fs", "tp"),
            P("fs", "tp"),
            P("fs", "tp"),
            P("fs", "tp"),
            P("tp"),
            P(("grp", "fs"), "tp"),
            P("tp"),
            P("tp", "fs"),
            P(),
            P(),
            P(),
            P("fs", "tp"),
            P("tp", "fs"),
        ),
        out_specs=P(("grp", "fs"), None),
        check_vma=False,
    )
```

```python
import functools

import jax
import jax.numpy as jnp
from jax import lax
from jax.experimental import pallas as pl
from jax.experimental.pallas import tpu as pltpu
from jax.sharding import PartitionSpec as P

DK = 64
DV = 128
SUB = 8

EPS = 1e-06
GATE_NORM_SCALE = 16.0
WEIGHT_SCALE = 2.0**16
HIGH = lax.Precision.HIGHEST
F32 = jnp.float32
BF16 = jnp.bfloat16


def root_norm(rows, gain):
    return rows * lax.rsqrt(jnp.mean(rows * rows, axis=-1, keepdims=True) + EPS) * gain


def attend_body(acc_ref, bias_ref, extra_ref, gain_ref, out_ref):
    length = acc_ref.shape[0]
    subs = length // SUB
    rounded = lambda lo, hi: acc_ref[:, lo:hi].astype(BF16).astype(F32)
    v = rounded(0, DV)
    g = rounded(DV, 2 * DV)
    q = rounded(2 * DV, 2 * DV + DK) * DK ** (-0.5)
    k = rounded(2 * DV + DK, 2 * DV + 2 * DK)
    pre = acc_ref[:, 2 * DV + 2 * DK : 2 * DV + 3 * DK] + bias_ref[...]
    log_sig = jnp.minimum(pre, 0.0) - jnp.log1p(jnp.exp(-jnp.abs(pre)))
    log_decay = log_sig / GATE_NORM_SCALE + extra_ref[...]
    row = lax.broadcasted_iota(jnp.int32, (length, length), 0)
    col = lax.broadcasted_iota(jnp.int32, (length, length), 1)
    dot = functools.partial(lax.dot_general, precision=HIGH, preferred_element_type=F32)
    nn, nt = (((1,), (0,)), ((), ())), (((1,), (1,)), ((), ()))
    cum = dot((row >= col).astype(F32), log_decay, nn)
    cum3, q3, k3 = (a.reshape(subs, SUB, DK) for a in (cum, q, k))
    inside = []
    for j in range(SUB):
        gap = jnp.minimum(cum3 - cum3[:, j : j + 1, :], 0.0)
        inside.append(jnp.sum(q3 * k3[:, j : j + 1, :] * jnp.exp(gap), axis=-1, keepdims=True))
    near = jnp.zeros((length, length), F32)
    for j in range(SUB):
        near = jnp.where(lax.rem(col, SUB) == j, inside[j].reshape(length, 1), near)
    same = (row // SUB == col // SUB) & (row >= col)
    far = [jnp.zeros((SUB, length), F32)]
    for i in range(1, subs):
        at = i * SUB
        mark = cum[at - 1 : at, :]
        left = q[at : at + SUB, :] * jnp.exp(jnp.minimum(cum[at : at + SUB, :] - mark, 0.0))
        right = k * jnp.exp(jnp.minimum(mark - cum, 0.0))
        far.append(dot(left, right, nt))
    scores = jnp.where(same, near, jnp.where(row // SUB > col // SUB, jnp.concatenate(far, 0), 0.0))
    attended = dot(scores, v, nn)
    scaled = attended * lax.rsqrt(jnp.mean(attended * attended, axis=-1, keepdims=True) + EPS)
    out_ref[...] = (scaled * gain_ref[...] * (g / (1.0 + jnp.exp(-g)))).astype(out_ref.dtype)


def attend(acc, bias, extra, gain):
    length = acc.shape[0]
    return pl.pallas_call(
        attend_body,
        out_shape=jax.ShapeDtypeStruct((length, DV), BF16),
        compiler_params=pltpu.CompilerParams(vmem_limit_bytes=16 * 2**20),
        cost_estimate=pl.CostEstimate(flops=40_000_000, bytes_accessed=500_000, transcendentals=400_000),
        name="attend",
    )(acc, bias, extra, gain)


def feed_body(halves, rows_ref, weight_ref, part_ref, out_ref, sum_ref, act_ref):
    step = pl.program_id(0)

    @pl.when(step < halves)
    def _():
        product = jnp.dot(rows_ref[...], weight_ref[...], preferred_element_type=F32)

        @pl.when(step == 0)
        def _():
            sum_ref[...] = product

        @pl.when(step > 0)
        def _():
            sum_ref[...] += product

        @pl.when(step == halves - 1)
        def _():
            act_ref[...] = jnp.square(jnp.maximum(sum_ref[...], 0.0)).astype(BF16)

    @pl.when(step >= halves)
    def _():
        product = lax.dot_general(
            act_ref[...], weight_ref[...], (((1,), (1,)), ((), ())), preferred_element_type=F32
        )
        out_ref[...] = (product + part_ref[...]).astype(out_ref.dtype)


def feed(rows, both, part):
    length, width = rows.shape
    units = both.shape[1] // 2
    halves = 2
    block = width // halves
    later = lambda s: (0, jnp.maximum(s - halves, 0))
    return pl.pallas_call(
        functools.partial(feed_body, halves),
        grid=(2 * halves,),
        in_specs=[
            pl.BlockSpec((length, block), lambda s: (0, jnp.minimum(s, halves - 1))),
            pl.BlockSpec((block, units), lambda s: (lax.rem(s, halves), s // halves)),
            pl.BlockSpec((length, block), later),
        ],
        out_specs=pl.BlockSpec((length, block), later),
        out_shape=jax.ShapeDtypeStruct((length, width), BF16),
        scratch_shapes=[pltpu.VMEM((length, units), F32), pltpu.VMEM((length, units), BF16)],
        compiler_params=pltpu.CompilerParams(
            dimension_semantics=("arbitrary",), vmem_limit_bytes=48 * 2**20
        ),
        cost_estimate=pl.CostEstimate(
            flops=4 * length * width * units, bytes_accessed=4 * width * units, transcendentals=0
        ),
        name="feed",
    )(rows, both, part)


def pack_body(first, up_ref, down_ref, out_ref, held, arrived, left):
    width = up_ref.shape[1] - first
    brought = []
    for i, source in enumerate((up_ref, down_ref)):
        copy = pltpu.make_async_copy(source.at[:, pl.ds(first, width)], held.at[i], arrived.at[i])
        copy.start()
        brought.append(copy)
    sent = []
    for i, copy in enumerate(brought):
        copy.wait()
        out = pltpu.make_async_copy(held.at[i], out_ref.at[:, pl.ds(i * width, width)], left.at[i])
        out.start()
        sent.append(out)
    for out in sent:
        out.wait()


def pack(up, down, first):
    depth, width = up.shape[0], up.shape[1] - first
    return pl.pallas_call(
        functools.partial(pack_body, first),
        in_specs=[pl.BlockSpec(memory_space=pltpu.HBM)] * 2,
        out_specs=pl.BlockSpec(memory_space=pltpu.HBM),
        out_shape=jax.ShapeDtypeStruct((depth, 2 * width), up.dtype),
        scratch_shapes=[
            pltpu.VMEM((2, depth, width), up.dtype),
            pltpu.SemaphoreType.DMA((2,)),
            pltpu.SemaphoreType.DMA((2,)),
        ],
        compiler_params=pltpu.CompilerParams(vmem_limit_bytes=62 * 2**20),
        name="pack",
    )(up, down)


def share_of_sum(part, axis):
    peers = lax.axis_size(axis)
    blocks = part.reshape(peers, part.shape[0] // peers, part.shape[1])
    arrived = lax.all_to_all(blocks, axis, split_axis=0, concat_axis=0, tiled=True)
    return arrived.astype(F32).sum(axis=0)


def local(
    tokens,
    pre_attention_gain,
    query_weight,
    key_weight,
    value_weight,
    output_gate_weight,
    decay_weight,
    decay_logit_bias,
    extra_log_decay,
    head_norm_gain,
    attention_out_weight,
    post_attention_gain,
    pre_feedforward_gain,
    post_feedforward_gain,
    up_weight,
    down_weight,
):
    apart = up_weight.shape[1] // 8
    down_rows = down_weight.T
    both = lax.all_gather(pack(up_weight, down_rows, apart), "fs", axis=0, tiled=True)
    groups = lax.axis_size("grp")
    side = lax.rem(lax.axis_index("grp"), 2)
    first = side == 0
    projections = jnp.concatenate(
        [value_weight, output_gate_weight, query_weight, key_weight, decay_weight], 1
    )
    parts = (up_weight[:, :apart], down_rows[:, :apart], projections, attention_out_weight.T)
    sizes = [p.shape[1] // 2 for p in parts]
    halves = [p[:, h * n : (h + 1) * n] for h in range(2) for p, n in zip(parts, sizes)]
    half = lax.dynamic_slice_in_dim(
        jnp.concatenate(halves, 1), side * sum(sizes), sum(sizes), 1
    )
    sent = (half.astype(F32) * WEIGHT_SCALE).astype(jnp.float16)
    held = lax.all_gather(sent, "fs", axis=0, tiled=True)
    tokens, held = lax.optimization_barrier((tokens, held))
    mine = (held.astype(F32) * (1.0 / WEIGHT_SCALE)).astype(BF16)
    swap = lambda w: lax.ppermute(w, "grp", [(i, i ^ 1) for i in range(groups)])
    edge = sizes[0] + sizes[1]
    near = mine[:, edge:]
    far = swap(near)
    apart_pair = (mine[:, :edge], swap(mine[:, :edge]))
    normed = root_norm(tokens.astype(F32), pre_attention_gain).astype(BF16)
    wide = sizes[2]
    acc_near, acc_far = (
        jnp.dot(normed, w[:, :wide], preferred_element_type=F32) for w in (near, far)
    )
    acc = jnp.concatenate(
        [jnp.where(first, acc_near, acc_far), jnp.where(first, acc_far, acc_near)], 1
    )
    headout = attend(acc, decay_logit_bias[None], extra_log_decay, head_norm_gain[None])

    low, high = headout[:, : sizes[3]], headout[:, sizes[3] :]
    mix_part = sum(
        lax.dot_general(h, w[:, wide:], (((1,), (1,)), ((), ())), preferred_element_type=F32)
        for h, w in ((jnp.where(first, low, high), near), (jnp.where(first, high, low), far))
    )
    mixed = share_of_sum(mix_part.astype(BF16), "tp")
    share = mixed.shape[0]
    own_tokens = lax.dynamic_slice_in_dim(tokens, lax.axis_index("tp") * share, share, 0)
    stream = own_tokens.astype(F32) + root_norm(mixed, post_attention_gain)
    normed_mid = root_norm(stream, pre_feedforward_gain).astype(BF16)
    rows = lax.all_gather(normed_mid, "tp", axis=0, tiled=True)
    part = 0.0
    for w in apart_pair:
        act = jnp.dot(rows, w[:, : sizes[0]], preferred_element_type=F32)
        act = jnp.square(jax.nn.relu(act)).astype(BF16)
        part += lax.dot_general(
            act, w[:, sizes[0] :], (((1,), (1,)), ((), ())), preferred_element_type=F32
        )
    feed_share = share_of_sum(feed(rows, both, part), "tp")
    out_share = (stream + root_norm(feed_share, post_feedforward_gain)).astype(BF16)
    return lax.all_gather(out_share, "tp", axis=0, tiled=True)


def solution(mesh):
    return jax.shard_map(
        local,
        mesh=mesh,
        in_specs=(
            P(("grp", "fs"), None),
            P(),
            P("fs", "tp"),
            P("fs", "tp"),
            P("fs", "tp"),
            P("fs", "tp"),
            P("fs", "tp"),
            P("tp"),
            P(("grp", "fs"), "tp"),
            P("tp"),
            P("tp", "fs"),
            P(),
            P(),
            P(),
            P("fs", "tp"),
            P("tp", "fs"),
        ),
        out_specs=P(("grp", "fs"), None),
        check_vma=False,
    )
```

```python
import functools

import jax
import jax.numpy as jnp
from jax import lax
from jax.experimental import pallas as pl
from jax.experimental.pallas import tpu as pltpu
from jax.sharding import PartitionSpec as P


DK = 64
DV = 128
SUB = 8

EPS = 1e-06
GATE_NORM_SCALE = 16.0
WEIGHT_SCALE = 2.0**16
HIGH = lax.Precision.HIGHEST
F32 = jnp.float32
BF16 = jnp.bfloat16


def root_norm(rows, gain):
    return rows * lax.rsqrt(jnp.mean(rows * rows, axis=-1, keepdims=True) + EPS) * gain


def attend_body(acc_ref, bias_ref, extra_ref, gain_ref, out_ref):
    length = acc_ref.shape[0]
    subs = length // SUB
    rounded = lambda lo, hi: acc_ref[:, lo:hi].astype(BF16).astype(F32)
    v = rounded(0, DV)
    g = rounded(DV, 2 * DV)
    q = rounded(2 * DV, 2 * DV + DK) * DK ** (-0.5)
    k = rounded(2 * DV + DK, 2 * DV + 2 * DK)
    pre = acc_ref[:, 2 * DV + 2 * DK : 2 * DV + 3 * DK] + bias_ref[...]
    log_sig = jnp.minimum(pre, 0.0) - jnp.log1p(jnp.exp(-jnp.abs(pre)))
    log_decay = log_sig / GATE_NORM_SCALE + extra_ref[...].T
    row = lax.broadcasted_iota(jnp.int32, (length, length), 0)
    col = lax.broadcasted_iota(jnp.int32, (length, length), 1)
    dot = functools.partial(lax.dot_general, precision=HIGH, preferred_element_type=F32)
    nn, nt = (((1,), (0,)), ((), ())), (((1,), (1,)), ((), ()))
    cum = dot((row >= col).astype(F32), log_decay, nn)
    cum3, q3, k3 = (a.reshape(subs, SUB, DK) for a in (cum, q, k))
    inside = []
    for j in range(SUB):
        gap = jnp.minimum(cum3 - cum3[:, j : j + 1, :], 0.0)
        inside.append(jnp.sum(q3 * k3[:, j : j + 1, :] * jnp.exp(gap), axis=-1, keepdims=True))
    near = jnp.zeros((length, length), F32)
    for j in range(SUB):
        near = jnp.where(lax.rem(col, SUB) == j, inside[j].reshape(length, 1), near)
    same = (row // SUB == col // SUB) & (row >= col)
    far = [jnp.zeros((SUB, length), F32)]
    for i in range(1, subs):
        at = i * SUB
        mark = cum[at - 1 : at, :]
        left = q[at : at + SUB, :] * jnp.exp(jnp.minimum(cum[at : at + SUB, :] - mark, 0.0))
        right = k * jnp.exp(jnp.minimum(mark - cum, 0.0))
        far.append(dot(left, right, nt))
    scores = jnp.where(same, near, jnp.where(row // SUB > col // SUB, jnp.concatenate(far, 0), 0.0))
    attended = dot(scores, v, nn)
    scaled = attended * lax.rsqrt(jnp.mean(attended * attended, axis=-1, keepdims=True) + EPS)
    out_ref[...] = (scaled * gain_ref[...] * (g / (1.0 + jnp.exp(-g)))).astype(out_ref.dtype)


def attend(acc, bias, extra, gain):
    length = acc.shape[0]
    return pl.pallas_call(
        attend_body,
        out_shape=jax.ShapeDtypeStruct((length, DV), BF16),
        compiler_params=pltpu.CompilerParams(vmem_limit_bytes=16 * 2**20),
        cost_estimate=pl.CostEstimate(flops=40_000_000, bytes_accessed=500_000, transcendentals=400_000),
        name="attend",
    )(acc, bias, extra, gain)


def feed_body(halves, rows_ref, weight_ref, part_ref, out_ref, sum_ref, act_ref):
    step = pl.program_id(0)

    @pl.when(step < halves)
    def _():
        product = jnp.dot(rows_ref[...], weight_ref[...], preferred_element_type=F32)

        @pl.when(step == 0)
        def _():
            sum_ref[...] = product

        @pl.when(step > 0)
        def _():
            sum_ref[...] += product

        @pl.when(step == halves - 1)
        def _():
            act_ref[...] = jnp.square(jnp.maximum(sum_ref[...], 0.0)).astype(BF16)

    @pl.when(step >= halves)
    def _():
        product = lax.dot_general(
            act_ref[...], weight_ref[...], (((1,), (1,)), ((), ())), preferred_element_type=F32
        )
        out_ref[...] = (product + part_ref[...]).astype(out_ref.dtype)


def feed(rows, both, part):
    length, width = rows.shape
    units = both.shape[1] // 2
    halves = 2
    block = width // halves
    later = lambda s: (0, jnp.maximum(s - halves, 0))
    return pl.pallas_call(
        functools.partial(feed_body, halves),
        grid=(2 * halves,),
        in_specs=[
            pl.BlockSpec((length, block), lambda s: (0, jnp.minimum(s, halves - 1))),
            pl.BlockSpec((block, units), lambda s: (lax.rem(s, halves), s // halves)),
            pl.BlockSpec((length, block), later),
        ],
        out_specs=pl.BlockSpec((length, block), later),
        out_shape=jax.ShapeDtypeStruct((length, width), BF16),
        scratch_shapes=[pltpu.VMEM((length, units), F32), pltpu.VMEM((length, units), BF16)],
        compiler_params=pltpu.CompilerParams(
            dimension_semantics=("arbitrary",), vmem_limit_bytes=48 * 2**20
        ),
        cost_estimate=pl.CostEstimate(
            flops=4 * length * width * units, bytes_accessed=4 * width * units, transcendentals=0
        ),
        name="feed",
    )(rows, both, part)


def pack_body(first, up_ref, down_ref, out_ref, held, arrived, left):
    width = up_ref.shape[1] - first
    brought = []
    for i, source in enumerate((up_ref, down_ref)):
        copy = pltpu.make_async_copy(source.at[:, pl.ds(first, width)], held.at[i], arrived.at[i])
        copy.start()
        brought.append(copy)
    sent = []
    for i, copy in enumerate(brought):
        copy.wait()
        out = pltpu.make_async_copy(held.at[i], out_ref.at[:, pl.ds(i * width, width)], left.at[i])
        out.start()
        sent.append(out)
    for out in sent:
        out.wait()


def pack(up, down, first):
    depth, width = up.shape[0], up.shape[1] - first
    return pl.pallas_call(
        functools.partial(pack_body, first),
        in_specs=[pl.BlockSpec(memory_space=pltpu.HBM)] * 2,
        out_specs=pl.BlockSpec(memory_space=pltpu.HBM),
        out_shape=jax.ShapeDtypeStruct((depth, 2 * width), up.dtype),
        scratch_shapes=[
            pltpu.VMEM((2, depth, width), up.dtype),
            pltpu.SemaphoreType.DMA((2,)),
            pltpu.SemaphoreType.DMA((2,)),
        ],
        compiler_params=pltpu.CompilerParams(vmem_limit_bytes=62 * 2**20),
        name="pack",
    )(up, down)


def share_of_sum(part, axis):
    peers = lax.axis_size(axis)
    blocks = part.reshape(peers, part.shape[0] // peers, part.shape[1])
    arrived = lax.all_to_all(blocks, axis, split_axis=0, concat_axis=0, tiled=True)
    return arrived.astype(F32).sum(axis=0)


def local(
    tokens,
    pre_attention_gain,
    query_weight,
    key_weight,
    value_weight,
    output_gate_weight,
    decay_weight,
    decay_logit_bias,
    extra_log_decay,
    head_norm_gain,
    attention_out_weight,
    post_attention_gain,
    pre_feedforward_gain,
    post_feedforward_gain,
    up_weight,
    down_weight,
):
    apart = up_weight.shape[1] // 8
    down_rows = down_weight.T
    both = lax.all_gather(pack(up_weight, down_rows, apart), "fs", axis=0, tiled=True)
    groups = lax.axis_size("grp")
    side = lax.rem(lax.axis_index("grp"), 2)
    first = side == 0
    projections = jnp.concatenate(
        [value_weight, output_gate_weight, query_weight, key_weight, decay_weight], 1
    )
    parts = (up_weight[:, :apart], down_rows[:, :apart], projections, attention_out_weight.T)
    sizes = [p.shape[1] // 2 for p in parts]
    halves = [p[:, h * n : (h + 1) * n] for h in range(2) for p, n in zip(parts, sizes)]
    half = lax.dynamic_slice_in_dim(
        jnp.concatenate(halves, 1), side * sum(sizes), sum(sizes), 1
    )
    sent = (half.astype(F32) * WEIGHT_SCALE).astype(jnp.float16)
    swap = lambda w: lax.ppermute(w, "grp", [(i, i ^ 1) for i in range(groups)])
    far_tokens = swap(tokens)
    held = lax.all_gather(sent, "fs", axis=0, tiled=True)
    far_tokens, held = lax.optimization_barrier((far_tokens, held))
    unscaled = lambda w, lo, hi: (w[:, lo:hi].astype(F32) * (1.0 / WEIGHT_SCALE)).astype(BF16)
    normed = lambda rows: root_norm(rows.astype(F32), pre_attention_gain).astype(BF16)
    edges = [sum(sizes[:i]) for i in range(5)]
    near = unscaled(held, edges[3], edges[4])
    far = swap(near)
    sent_home = jnp.dot(
        normed(far_tokens), unscaled(held, edges[2], edges[3]), preferred_element_type=F32
    )
    acc_far = swap(sent_home)
    tokens, held, sent_home = lax.optimization_barrier((tokens, held, sent_home))
    acc_near = jnp.dot(
        normed(tokens), unscaled(held, edges[2], edges[3]), preferred_element_type=F32
    )
    acc = jnp.concatenate(
        [jnp.where(first, acc_near, acc_far), jnp.where(first, acc_far, acc_near)], 1
    )
    headout = attend(acc, decay_logit_bias[None], extra_log_decay.T, head_norm_gain[None])

    low, high = headout[:, : sizes[3]], headout[:, sizes[3] :]
    mix_part = sum(
        lax.dot_general(h, w, (((1,), (1,)), ((), ())), preferred_element_type=F32)
        for h, w in ((jnp.where(first, low, high), near), (jnp.where(first, high, low), far))
    )
    mix_part, held = lax.optimization_barrier((mix_part.astype(BF16), held))
    mixed = share_of_sum(mix_part, "tp")
    apart_near = unscaled(held, 0, edges[2])
    apart_far = swap(apart_near)
    up_apart, down_apart = (
        jnp.concatenate([w[:, lo:hi] for w in (apart_near, apart_far)], 1)
        for lo, hi in zip(edges[:2], edges[1:3])
    )
    share = mixed.shape[0]
    own_tokens = lax.dynamic_slice_in_dim(tokens, lax.axis_index("tp") * share, share, 0)
    stream = own_tokens.astype(F32) + root_norm(mixed, post_attention_gain)
    normed_mid = root_norm(stream, pre_feedforward_gain).astype(BF16)
    rows = lax.all_gather(normed_mid, "tp", axis=0, tiled=True)
    act = jnp.square(jax.nn.relu(jnp.dot(rows, up_apart, preferred_element_type=F32))).astype(BF16)
    part = lax.dot_general(act, down_apart, (((1,), (1,)), ((), ())), preferred_element_type=F32)
    feed_share = share_of_sum(feed(rows, both, part), "tp")
    out_share = (stream + root_norm(feed_share, post_feedforward_gain)).astype(BF16)
    return lax.all_gather(out_share, "tp", axis=0, tiled=True)


def solution(mesh):
    return jax.shard_map(
        local,
        mesh=mesh,
        in_specs=(
            P(("grp", "fs"), None),
            P(),
            P("fs", "tp"),
            P("fs", "tp"),
            P("fs", "tp"),
            P("fs", "tp"),
            P("fs", "tp"),
            P("tp"),
            P(("grp", "fs"), "tp"),
            P("tp"),
            P("tp", "fs"),
            P(),
            P(),
            P(),
            P("fs", "tp"),
            P("tp", "fs"),
        ),
        out_specs=P(("grp", "fs"), None),
        check_vma=False,
    )
```

```python
import functools

import jax
import jax.numpy as jnp
from jax import lax
from jax.experimental import pallas as pl
from jax.experimental.layout import Layout, with_layout_constraint
from jax.experimental.pallas import tpu as pltpu
from jax.sharding import PartitionSpec as P


DK = 64
DV = 128
SUB = 8

EPS = 1e-06
GATE_NORM_SCALE = 16.0
WEIGHT_SCALE = 2.0**16
HIGH = lax.Precision.HIGHEST
F32 = jnp.float32
BF16 = jnp.bfloat16


def root_norm(rows, gain):
    return rows * lax.rsqrt(jnp.mean(rows * rows, axis=-1, keepdims=True) + EPS) * gain


def attend_body(acc_ref, bias_ref, extra_ref, gain_ref, out_ref):
    length = acc_ref.shape[0]
    subs = length // SUB
    rounded = lambda lo, hi: acc_ref[:, lo:hi].astype(BF16).astype(F32)
    v = rounded(0, DV)
    g = rounded(DV, 2 * DV)
    q = rounded(2 * DV, 2 * DV + DK) * DK ** (-0.5)
    k = rounded(2 * DV + DK, 2 * DV + 2 * DK)
    pre = acc_ref[:, 2 * DV + 2 * DK : 2 * DV + 3 * DK] + bias_ref[...]
    log_sig = jnp.minimum(pre, 0.0) - jnp.log1p(jnp.exp(-jnp.abs(pre)))
    log_decay = log_sig / GATE_NORM_SCALE + extra_ref[...].T
    row = lax.broadcasted_iota(jnp.int32, (length, length), 0)
    col = lax.broadcasted_iota(jnp.int32, (length, length), 1)
    dot = functools.partial(lax.dot_general, precision=HIGH, preferred_element_type=F32)
    nn, nt = (((1,), (0,)), ((), ())), (((1,), (1,)), ((), ()))
    cum = dot((row >= col).astype(F32), log_decay, nn)
    cum3, q3, k3 = (a.reshape(subs, SUB, DK) for a in (cum, q, k))
    inside = []
    for j in range(SUB):
        gap = jnp.minimum(cum3 - cum3[:, j : j + 1, :], 0.0)
        inside.append(jnp.sum(q3 * k3[:, j : j + 1, :] * jnp.exp(gap), axis=-1, keepdims=True))
    near = jnp.zeros((length, length), F32)
    for j in range(SUB):
        near = jnp.where(lax.rem(col, SUB) == j, inside[j].reshape(length, 1), near)
    same = (row // SUB == col // SUB) & (row >= col)
    far = [jnp.zeros((SUB, length), F32)]
    for i in range(1, subs):
        at = i * SUB
        mark = cum[at - 1 : at, :]
        left = q[at : at + SUB, :] * jnp.exp(jnp.minimum(cum[at : at + SUB, :] - mark, 0.0))
        right = k * jnp.exp(jnp.minimum(mark - cum, 0.0))
        far.append(dot(left, right, nt))
    scores = jnp.where(same, near, jnp.where(row // SUB > col // SUB, jnp.concatenate(far, 0), 0.0))
    attended = dot(scores, v, nn)
    scaled = attended * lax.rsqrt(jnp.mean(attended * attended, axis=-1, keepdims=True) + EPS)
    out_ref[...] = (scaled * gain_ref[...] * (g / (1.0 + jnp.exp(-g)))).astype(out_ref.dtype)


def attend(acc, bias, extra, gain):
    length = acc.shape[0]
    return pl.pallas_call(
        attend_body,
        out_shape=jax.ShapeDtypeStruct((length, DV), BF16),
        compiler_params=pltpu.CompilerParams(vmem_limit_bytes=16 * 2**20),
        cost_estimate=pl.CostEstimate(flops=40_000_000, bytes_accessed=500_000, transcendentals=400_000),
        name="attend",
    )(acc, bias, extra, gain)


def feed_body(halves, rows_ref, weight_ref, part_ref, out_ref, sum_ref, act_ref):
    step = pl.program_id(0)

    @pl.when(step < halves)
    def _():
        product = jnp.dot(rows_ref[...], weight_ref[...], preferred_element_type=F32)

        @pl.when(step == 0)
        def _():
            sum_ref[...] = product

        @pl.when(step > 0)
        def _():
            sum_ref[...] += product

        @pl.when(step == halves - 1)
        def _():
            act_ref[...] = jnp.square(jnp.maximum(sum_ref[...], 0.0)).astype(BF16)

    @pl.when(step >= halves)
    def _():
        product = lax.dot_general(
            act_ref[...], weight_ref[...], (((1,), (1,)), ((), ())), preferred_element_type=F32
        )
        out_ref[...] = (product + part_ref[...]).astype(out_ref.dtype)


def feed(rows, both, part):
    length, width = rows.shape
    units = both.shape[1] // 2
    halves = 2
    block = width // halves
    later = lambda s: (0, jnp.maximum(s - halves, 0))
    return pl.pallas_call(
        functools.partial(feed_body, halves),
        grid=(2 * halves,),
        in_specs=[
            pl.BlockSpec((length, block), lambda s: (0, jnp.minimum(s, halves - 1))),
            pl.BlockSpec((block, units), lambda s: (lax.rem(s, halves), s // halves)),
            pl.BlockSpec((length, block), later),
        ],
        out_specs=pl.BlockSpec((length, block), later),
        out_shape=jax.ShapeDtypeStruct((length, width), BF16),
        scratch_shapes=[pltpu.VMEM((length, units), F32), pltpu.VMEM((length, units), BF16)],
        compiler_params=pltpu.CompilerParams(
            dimension_semantics=("arbitrary",), vmem_limit_bytes=48 * 2**20
        ),
        cost_estimate=pl.CostEstimate(
            flops=4 * length * width * units, bytes_accessed=4 * width * units, transcendentals=0
        ),
        name="feed",
    )(rows, both, part)


def pack_body(first, up_ref, down_ref, out_ref, held, arrived, left):
    width = up_ref.shape[1] - first
    brought = []
    for i, source in enumerate((up_ref, down_ref)):
        copy = pltpu.make_async_copy(source.at[:, pl.ds(first, width)], held.at[i], arrived.at[i])
        copy.start()
        brought.append(copy)
    sent = []
    for i, copy in enumerate(brought):
        copy.wait()
        out = pltpu.make_async_copy(held.at[i], out_ref.at[:, pl.ds(i * width, width)], left.at[i])
        out.start()
        sent.append(out)
    for out in sent:
        out.wait()


def pack(up, down, first):
    depth, width = up.shape[0], up.shape[1] - first
    return pl.pallas_call(
        functools.partial(pack_body, first),
        in_specs=[pl.BlockSpec(memory_space=pltpu.HBM)] * 2,
        out_specs=pl.BlockSpec(memory_space=pltpu.HBM),
        out_shape=jax.ShapeDtypeStruct((depth, 2 * width), up.dtype),
        scratch_shapes=[
            pltpu.VMEM((2, depth, width), up.dtype),
            pltpu.SemaphoreType.DMA((2,)),
            pltpu.SemaphoreType.DMA((2,)),
        ],
        compiler_params=pltpu.CompilerParams(vmem_limit_bytes=62 * 2**20),
        name="pack",
    )(up, down)


def share_of_sum(part, axis):
    peers = lax.axis_size(axis)
    blocks = part.reshape(peers, part.shape[0] // peers, part.shape[1])
    arrived = lax.all_to_all(blocks, axis, split_axis=0, concat_axis=0, tiled=True)
    return arrived.astype(F32).sum(axis=0)


def local(
    tokens,
    pre_attention_gain,
    query_weight,
    key_weight,
    value_weight,
    output_gate_weight,
    decay_weight,
    decay_logit_bias,
    extra_log_decay,
    head_norm_gain,
    attention_out_weight,
    post_attention_gain,
    pre_feedforward_gain,
    post_feedforward_gain,
    up_weight,
    down_weight,
):
    apart = up_weight.shape[1] // 8
    down_rows = down_weight.T
    both = lax.all_gather(pack(up_weight, down_rows, apart), "fs", axis=0, tiled=True)
    groups = lax.axis_size("grp")
    side = lax.rem(lax.axis_index("grp"), 2)
    first = side == 0
    projections = jnp.concatenate(
        [value_weight, output_gate_weight, query_weight, key_weight, decay_weight], 1
    )
    parts = (up_weight[:, :apart], down_rows[:, :apart], projections, attention_out_weight.T)
    sizes = [p.shape[1] // 2 for p in parts]
    halves = [p[:, h * n : (h + 1) * n] for h in range(2) for p, n in zip(parts, sizes)]
    half = lax.dynamic_slice_in_dim(
        jnp.concatenate(halves, 1), side * sum(sizes), sum(sizes), 1
    )
    sent = (half.astype(F32) * WEIGHT_SCALE).astype(jnp.float16)
    swap = lambda w: lax.ppermute(w, "grp", [(i, i ^ 1) for i in range(groups)])
    far_tokens = swap(tokens)
    held = lax.all_gather(sent, "fs", axis=0, tiled=True)
    far_tokens, held = lax.optimization_barrier((far_tokens, held))
    unscaled = lambda w, lo, hi: (w[:, lo:hi].astype(F32) * (1.0 / WEIGHT_SCALE)).astype(BF16)
    normed = lambda rows: root_norm(rows.astype(F32), pre_attention_gain).astype(BF16)
    edges = [sum(sizes[:i]) for i in range(5)]
    sent_home = jnp.dot(
        normed(far_tokens), unscaled(held, edges[2], edges[3]), preferred_element_type=F32
    )
    acc_far = swap(sent_home)
    tokens, held, sent_home = lax.optimization_barrier((tokens, held, sent_home))
    acc_near = jnp.dot(
        normed(tokens), unscaled(held, edges[2], edges[3]), preferred_element_type=F32
    )
    dense = lambda w: with_layout_constraint(w, Layout(major_to_minor=(0, 1)))
    near = dense(dense(unscaled(held, edges[3], edges[4])).T)
    far = dense(swap(near))
    acc = jnp.concatenate(
        [jnp.where(first, acc_near, acc_far), jnp.where(first, acc_far, acc_near)], 1
    )
    headout = attend(acc, decay_logit_bias[None], extra_log_decay.T, head_norm_gain[None])

    low, high = headout[:, : sizes[3]], headout[:, sizes[3] :]
    mix_part = sum(
        jnp.dot(h, w, preferred_element_type=F32)
        for h, w in ((jnp.where(first, low, high), near), (jnp.where(first, high, low), far))
    )
    mix_part, held = lax.optimization_barrier((mix_part.astype(BF16), held))
    mixed = share_of_sum(mix_part, "tp")
    apart_near = unscaled(held, 0, edges[2])
    apart_far = swap(apart_near)
    up_apart, down_apart = (
        jnp.concatenate([w[:, lo:hi] for w in (apart_near, apart_far)], 1)
        for lo, hi in zip(edges[:2], edges[1:3])
    )
    share = mixed.shape[0]
    own_tokens = lax.dynamic_slice_in_dim(tokens, lax.axis_index("tp") * share, share, 0)
    stream = own_tokens.astype(F32) + root_norm(mixed, post_attention_gain)
    normed_mid = root_norm(stream, pre_feedforward_gain).astype(BF16)
    rows = lax.all_gather(normed_mid, "tp", axis=0, tiled=True)
    act = jnp.square(jax.nn.relu(jnp.dot(rows, up_apart, preferred_element_type=F32))).astype(BF16)
    part = lax.dot_general(act, down_apart, (((1,), (1,)), ((), ())), preferred_element_type=F32)
    feed_share = share_of_sum(feed(rows, both, part), "tp")
    out_share = (stream + root_norm(feed_share, post_feedforward_gain)).astype(BF16)
    return lax.all_gather(out_share, "tp", axis=0, tiled=True)


def solution(mesh):
    return jax.shard_map(
        local,
        mesh=mesh,
        in_specs=(
            P(("grp", "fs"), None),
            P(),
            P("fs", "tp"),
            P("fs", "tp"),
            P("fs", "tp"),
            P("fs", "tp"),
            P("fs", "tp"),
            P("tp"),
            P(("grp", "fs"), "tp"),
            P("tp"),
            P("tp", "fs"),
            P(),
            P(),
            P(),
            P("fs", "tp"),
            P("tp", "fs"),
        ),
        out_specs=P(("grp", "fs"), None),
        check_vma=False,
    )
```

```python
import functools

import jax
import jax.numpy as jnp
from jax import lax
from jax.experimental import pallas as pl
from jax.experimental.layout import Layout, with_layout_constraint
from jax.experimental.pallas import tpu as pltpu
from jax.sharding import PartitionSpec as P


DK = 64
DV = 128
SUB = 8

EPS = 1e-06
GATE_NORM_SCALE = 16.0
WEIGHT_SCALE = 2.0**16
HIGH = lax.Precision.HIGHEST
F32 = jnp.float32
BF16 = jnp.bfloat16


def root_norm(rows, gain):
    return rows * lax.rsqrt(jnp.mean(rows * rows, axis=-1, keepdims=True) + EPS) * gain


def attend_body(acc_ref, bias_ref, extra_ref, gain_ref, out_ref):
    length = acc_ref.shape[0]
    subs = length // SUB
    rounded = lambda lo, hi: acc_ref[:, lo:hi].astype(BF16).astype(F32)
    v = rounded(0, DV)
    g = rounded(DV, 2 * DV)
    q = rounded(2 * DV, 2 * DV + DK) * DK ** (-0.5)
    k = rounded(2 * DV + DK, 2 * DV + 2 * DK)
    pre = acc_ref[:, 2 * DV + 2 * DK : 2 * DV + 3 * DK] + bias_ref[...]
    log_sig = jnp.minimum(pre, 0.0) - jnp.log1p(jnp.exp(-jnp.abs(pre)))
    log_decay = log_sig / GATE_NORM_SCALE + extra_ref[...].T
    row = lax.broadcasted_iota(jnp.int32, (length, length), 0)
    col = lax.broadcasted_iota(jnp.int32, (length, length), 1)
    dot = functools.partial(lax.dot_general, precision=HIGH, preferred_element_type=F32)
    nn, nt = (((1,), (0,)), ((), ())), (((1,), (1,)), ((), ()))
    cum = dot((row >= col).astype(F32), log_decay, nn)
    cum3, q3, k3 = (a.reshape(subs, SUB, DK) for a in (cum, q, k))
    inside = []
    for j in range(SUB):
        gap = jnp.minimum(cum3 - cum3[:, j : j + 1, :], 0.0)
        inside.append(jnp.sum(q3 * k3[:, j : j + 1, :] * jnp.exp(gap), axis=-1, keepdims=True))
    near = jnp.zeros((length, length), F32)
    for j in range(SUB):
        near = jnp.where(lax.rem(col, SUB) == j, inside[j].reshape(length, 1), near)
    same = (row // SUB == col // SUB) & (row >= col)
    far = [jnp.zeros((SUB, length), F32)]
    for i in range(1, subs):
        at = i * SUB
        mark = cum[at - 1 : at, :]
        left = q[at : at + SUB, :] * jnp.exp(jnp.minimum(cum[at : at + SUB, :] - mark, 0.0))
        right = k * jnp.exp(jnp.minimum(mark - cum, 0.0))
        far.append(dot(left, right, nt))
    scores = jnp.where(same, near, jnp.where(row // SUB > col // SUB, jnp.concatenate(far, 0), 0.0))
    attended = dot(scores, v, nn)
    scaled = attended * lax.rsqrt(jnp.mean(attended * attended, axis=-1, keepdims=True) + EPS)
    out_ref[...] = (scaled * gain_ref[...] * (g / (1.0 + jnp.exp(-g)))).astype(out_ref.dtype)


def attend(acc, bias, extra, gain):
    length = acc.shape[0]
    return pl.pallas_call(
        attend_body,
        out_shape=jax.ShapeDtypeStruct((length, DV), BF16),
        compiler_params=pltpu.CompilerParams(vmem_limit_bytes=16 * 2**20),
        cost_estimate=pl.CostEstimate(flops=40_000_000, bytes_accessed=500_000, transcendentals=400_000),
        name="attend",
    )(acc, bias, extra, gain)


def feed_body(halves, rows_ref, weight_ref, part_ref, out_ref, sum_ref, act_ref):
    step = pl.program_id(0)

    @pl.when(step < halves)
    def _():
        product = jnp.dot(rows_ref[...], weight_ref[...], preferred_element_type=F32)

        @pl.when(step == 0)
        def _():
            sum_ref[...] = product

        @pl.when(step > 0)
        def _():
            sum_ref[...] += product

        @pl.when(step == halves - 1)
        def _():
            act_ref[...] = jnp.square(jnp.maximum(sum_ref[...], 0.0)).astype(BF16)

    @pl.when(step >= halves)
    def _():
        product = lax.dot_general(
            act_ref[...], weight_ref[...], (((1,), (1,)), ((), ())), preferred_element_type=F32
        )
        out_ref[...] = (product + part_ref[...]).astype(out_ref.dtype)


def feed(rows, both, part):
    length, width = rows.shape
    units = both.shape[1] // 2
    halves = 2
    block = width // halves
    later = lambda s: (0, jnp.maximum(s - halves, 0))
    return pl.pallas_call(
        functools.partial(feed_body, halves),
        grid=(2 * halves,),
        in_specs=[
            pl.BlockSpec((length, block), lambda s: (0, jnp.minimum(s, halves - 1))),
            pl.BlockSpec((block, units), lambda s: (lax.rem(s, halves), s // halves)),
            pl.BlockSpec((length, block), later),
        ],
        out_specs=pl.BlockSpec((length, block), later),
        out_shape=jax.ShapeDtypeStruct((length, width), BF16),
        scratch_shapes=[pltpu.VMEM((length, units), F32), pltpu.VMEM((length, units), BF16)],
        compiler_params=pltpu.CompilerParams(
            dimension_semantics=("arbitrary",), vmem_limit_bytes=48 * 2**20
        ),
        cost_estimate=pl.CostEstimate(
            flops=4 * length * width * units, bytes_accessed=4 * width * units, transcendentals=0
        ),
        name="feed",
    )(rows, both, part)


def pack_body(first, up_ref, down_ref, out_ref, held, arrived, left):
    width = up_ref.shape[1] - first
    brought = []
    for i, source in enumerate((up_ref, down_ref)):
        copy = pltpu.make_async_copy(source.at[:, pl.ds(first, width)], held.at[i], arrived.at[i])
        copy.start()
        brought.append(copy)
    sent = []
    for i, copy in enumerate(brought):
        copy.wait()
        out = pltpu.make_async_copy(held.at[i], out_ref.at[:, pl.ds(i * width, width)], left.at[i])
        out.start()
        sent.append(out)
    for out in sent:
        out.wait()


def pack(up, down, first):
    depth, width = up.shape[0], up.shape[1] - first
    return pl.pallas_call(
        functools.partial(pack_body, first),
        in_specs=[pl.BlockSpec(memory_space=pltpu.HBM)] * 2,
        out_specs=pl.BlockSpec(memory_space=pltpu.HBM),
        out_shape=jax.ShapeDtypeStruct((depth, 2 * width), up.dtype),
        scratch_shapes=[
            pltpu.VMEM((2, depth, width), up.dtype),
            pltpu.SemaphoreType.DMA((2,)),
            pltpu.SemaphoreType.DMA((2,)),
        ],
        compiler_params=pltpu.CompilerParams(vmem_limit_bytes=62 * 2**20),
        name="pack",
    )(up, down)


def share_of_sum(part, axis):
    peers = lax.axis_size(axis)
    blocks = part.reshape(peers, part.shape[0] // peers, part.shape[1])
    arrived = lax.all_to_all(blocks, axis, split_axis=0, concat_axis=0, tiled=True)
    return arrived.astype(F32).sum(axis=0)


def local(
    tokens,
    pre_attention_gain,
    query_weight,
    key_weight,
    value_weight,
    output_gate_weight,
    decay_weight,
    decay_logit_bias,
    extra_log_decay,
    head_norm_gain,
    attention_out_weight,
    post_attention_gain,
    pre_feedforward_gain,
    post_feedforward_gain,
    up_weight,
    down_weight,
):
    apart = up_weight.shape[1] // 8
    down_rows = down_weight.T
    both = lax.all_gather(pack(up_weight, down_rows, apart), "fs", axis=0, tiled=True)
    groups = lax.axis_size("grp")
    side = lax.rem(lax.axis_index("grp"), 2)
    first = side == 0
    projections = jnp.concatenate(
        [value_weight, output_gate_weight, query_weight, key_weight, decay_weight], 1
    )
    parts = (up_weight[:, :apart], down_rows[:, :apart], projections, attention_out_weight.T)
    sizes = [p.shape[1] // 2 for p in parts]
    halves = [p[:, h * n : (h + 1) * n] for h in range(2) for p, n in zip(parts, sizes)]
    half = lax.dynamic_slice_in_dim(
        jnp.concatenate(halves, 1), side * sum(sizes), sum(sizes), 1
    )
    sent = (half.astype(F32) * WEIGHT_SCALE).astype(jnp.float16)
    swap = lambda w: lax.ppermute(w, "grp", [(i, i ^ 1) for i in range(groups)])
    far_tokens = swap(tokens)
    held = lax.all_gather(sent, "fs", axis=0, tiled=True)
    far_tokens, held = lax.optimization_barrier((far_tokens, held))
    unscaled = lambda w, lo, hi: (w[:, lo:hi].astype(F32) * (1.0 / WEIGHT_SCALE)).astype(BF16)
    normed = lambda rows: root_norm(rows.astype(F32), pre_attention_gain).astype(BF16)
    edges = [sum(sizes[:i]) for i in range(5)]
    sent_home = jnp.dot(
        normed(far_tokens), unscaled(held, edges[2], edges[3]), preferred_element_type=F32
    )
    acc_far = swap(sent_home)
    tokens, held, sent_home = lax.optimization_barrier((tokens, held, sent_home))
    share = tokens.shape[0] // lax.axis_size("tp")
    own_tokens = lax.dynamic_slice_in_dim(tokens, lax.axis_index("tp") * share, share, 0)
    own_tokens = lax.optimization_barrier(own_tokens.astype(F32))
    acc_near = jnp.dot(
        normed(tokens), unscaled(held, edges[2], edges[3]), preferred_element_type=F32
    )
    dense = lambda w: with_layout_constraint(w, Layout(major_to_minor=(0, 1)))
    near = dense(dense(unscaled(held, edges[3], edges[4])).T)
    far = dense(swap(near))
    acc = jnp.concatenate(
        [jnp.where(first, acc_near, acc_far), jnp.where(first, acc_far, acc_near)], 1
    )
    headout = attend(acc, decay_logit_bias[None], extra_log_decay.T, head_norm_gain[None])

    low, high = headout[:, : sizes[3]], headout[:, sizes[3] :]
    mix_part = sum(
        jnp.dot(h, w, preferred_element_type=F32)
        for h, w in ((jnp.where(first, low, high), near), (jnp.where(first, high, low), far))
    )
    mix_part, held = lax.optimization_barrier((mix_part.astype(BF16), held))
    mixed = share_of_sum(mix_part, "tp")
    apart_near = unscaled(held, 0, edges[2])
    apart_far = swap(apart_near)
    up_apart, down_apart = (
        jnp.concatenate([w[:, lo:hi] for w in (apart_near, apart_far)], 1)
        for lo, hi in zip(edges[:2], edges[1:3])
    )
    stream = own_tokens + root_norm(mixed, post_attention_gain)
    normed_mid = root_norm(stream, pre_feedforward_gain).astype(BF16)
    rows = lax.all_gather(normed_mid, "tp", axis=0, tiled=True)
    act = jnp.square(jax.nn.relu(jnp.dot(rows, up_apart, preferred_element_type=F32))).astype(BF16)
    part = lax.dot_general(act, down_apart, (((1,), (1,)), ((), ())), preferred_element_type=F32)
    feed_share = share_of_sum(feed(rows, both, part), "tp")
    out_share = (stream + root_norm(feed_share, post_feedforward_gain)).astype(BF16)
    return lax.all_gather(out_share, "tp", axis=0, tiled=True)


def solution(mesh):
    return jax.shard_map(
        local,
        mesh=mesh,
        in_specs=(
            P(("grp", "fs"), None),
            P(),
            P("fs", "tp"),
            P("fs", "tp"),
            P("fs", "tp"),
            P("fs", "tp"),
            P("fs", "tp"),
            P("tp"),
            P(("grp", "fs"), "tp"),
            P("tp"),
            P("tp", "fs"),
            P(),
            P(),
            P(),
            P("fs", "tp"),
            P("tp", "fs"),
        ),
        out_specs=P(("grp", "fs"), None),
        check_vma=False,
    )
```

```python
import functools

import jax
import jax.numpy as jnp
from jax import lax
from jax.experimental import pallas as pl
from jax.experimental.layout import Layout, with_layout_constraint
from jax.experimental.pallas import tpu as pltpu
from jax.sharding import PartitionSpec as P


DK = 64
DV = 128
SUB = 8

EPS = 1e-06
GATE_NORM_SCALE = 16.0
WEIGHT_SCALE = 2.0**16
HIGH = lax.Precision.HIGHEST
F32 = jnp.float32
BF16 = jnp.bfloat16


def root_norm(rows, gain):
    return rows * lax.rsqrt(jnp.mean(rows * rows, axis=-1, keepdims=True) + EPS) * gain


def attend_body(acc_ref, bias_ref, extra_ref, gain_ref, out_ref):
    length = acc_ref.shape[0]
    subs = length // SUB
    rounded = lambda lo, hi: acc_ref[:, lo:hi].astype(BF16).astype(F32)
    v = rounded(0, DV)
    g = rounded(DV, 2 * DV)
    q = rounded(2 * DV, 2 * DV + DK) * DK ** (-0.5)
    k = rounded(2 * DV + DK, 2 * DV + 2 * DK)
    pre = acc_ref[:, 2 * DV + 2 * DK : 2 * DV + 3 * DK] + bias_ref[...]
    log_sig = jnp.minimum(pre, 0.0) - jnp.log1p(jnp.exp(-jnp.abs(pre)))
    log_decay = log_sig / GATE_NORM_SCALE + extra_ref[...].T
    row = lax.broadcasted_iota(jnp.int32, (length, length), 0)
    col = lax.broadcasted_iota(jnp.int32, (length, length), 1)
    dot = functools.partial(lax.dot_general, precision=HIGH, preferred_element_type=F32)
    nn, nt = (((1,), (0,)), ((), ())), (((1,), (1,)), ((), ()))
    cum = dot((row >= col).astype(F32), log_decay, nn)
    cum3, q3, k3 = (a.reshape(subs, SUB, DK) for a in (cum, q, k))
    inside = []
    for j in range(SUB):
        gap = jnp.minimum(cum3 - cum3[:, j : j + 1, :], 0.0)
        inside.append(jnp.sum(q3 * k3[:, j : j + 1, :] * jnp.exp(gap), axis=-1, keepdims=True))
    near = jnp.zeros((length, length), F32)
    for j in range(SUB):
        near = jnp.where(lax.rem(col, SUB) == j, inside[j].reshape(length, 1), near)
    same = (row // SUB == col // SUB) & (row >= col)
    far = [jnp.zeros((SUB, length), F32)]
    for i in range(1, subs):
        at = i * SUB
        mark = cum[at - 1 : at, :]
        left = q[at : at + SUB, :] * jnp.exp(jnp.minimum(cum[at : at + SUB, :] - mark, 0.0))
        right = k * jnp.exp(jnp.minimum(mark - cum, 0.0))
        far.append(dot(left, right, nt))
    scores = jnp.where(same, near, jnp.where(row // SUB > col // SUB, jnp.concatenate(far, 0), 0.0))
    attended = dot(scores, v, nn)
    scaled = attended * lax.rsqrt(jnp.mean(attended * attended, axis=-1, keepdims=True) + EPS)
    out_ref[...] = (scaled * gain_ref[...] * (g / (1.0 + jnp.exp(-g)))).astype(out_ref.dtype)


def attend(acc, bias, extra, gain):
    length = acc.shape[0]
    return pl.pallas_call(
        attend_body,
        out_shape=jax.ShapeDtypeStruct((length, DV), BF16),
        compiler_params=pltpu.CompilerParams(vmem_limit_bytes=16 * 2**20),
        cost_estimate=pl.CostEstimate(flops=40_000_000, bytes_accessed=500_000, transcendentals=400_000),
        name="attend",
    )(acc, bias, extra, gain)


def feed_body(
    halves, rows_ref, weight_ref, last_ref, early_ref, part_ref, out_ref, sum_ref, act_ref
):
    step = pl.program_id(0)

    @pl.when(step < halves)
    def _():
        product = jnp.dot(rows_ref[...], weight_ref[...], preferred_element_type=F32)

        @pl.when(step == 0)
        def _():
            sum_ref[...] = product

        @pl.when(step > 0)
        def _():
            sum_ref[...] += product

        @pl.when(step == halves - 1)
        def _():
            act_ref[...] = jnp.square(jnp.maximum(sum_ref[...], 0.0)).astype(BF16)

    @pl.when(step >= halves)
    def _():
        product = lax.dot_general(
            act_ref[...], weight_ref[...], (((1,), (1,)), ((), ())), preferred_element_type=F32
        )
        product += lax.dot_general(
            early_ref[...], last_ref[...], (((1,), (1,)), ((), ())), preferred_element_type=F32
        )
        out_ref[...] = (product + part_ref[...]).astype(out_ref.dtype)


def feed(rows, both, early, part):
    length, width = rows.shape
    count = early.shape[1]
    units = (both.shape[1] - count) // 2
    halves = 2
    block = width // halves
    later = lambda s: (0, jnp.maximum(s - halves, 0))
    return pl.pallas_call(
        functools.partial(feed_body, halves),
        grid=(2 * halves,),
        in_specs=[
            pl.BlockSpec((length, block), lambda s: (0, jnp.minimum(s, halves - 1))),
            pl.BlockSpec((block, units), lambda s: (lax.rem(s, halves), s // halves)),
            pl.BlockSpec(
                (block, count), lambda s: (jnp.maximum(s - halves, 0), 2 * units // count)
            ),
            pl.BlockSpec((length, count), lambda s: (0, 0)),
            pl.BlockSpec((length, block), later),
        ],
        out_specs=pl.BlockSpec((length, block), later),
        out_shape=jax.ShapeDtypeStruct((length, width), BF16),
        scratch_shapes=[pltpu.VMEM((length, units), F32), pltpu.VMEM((length, units), BF16)],
        compiler_params=pltpu.CompilerParams(
            dimension_semantics=("arbitrary",), vmem_limit_bytes=48 * 2**20
        ),
        cost_estimate=pl.CostEstimate(
            flops=4 * length * width * units, bytes_accessed=4 * width * units, transcendentals=0
        ),
        name="feed",
    )(rows, both, both, early, part)


def pack_body(first, up_ref, down_ref, out_ref, held, arrived, left):
    most = up_ref.shape[1] - 2 * first
    plan = (
        (up_ref, 2 * first, most, 0),
        (down_ref, 2 * first, most, most),
        (down_ref, first, first, 2 * most),
    )
    brought = []
    for i, (source, at, width, to) in enumerate(plan):
        copy = pltpu.make_async_copy(
            source.at[:, pl.ds(at, width)], held.at[:, pl.ds(to, width)], arrived.at[i]
        )
        copy.start()
        brought.append(copy)
    sent = []
    for i, (source, at, width, to) in enumerate(plan):
        brought[i].wait()
        out = pltpu.make_async_copy(
            held.at[:, pl.ds(to, width)], out_ref.at[:, pl.ds(to, width)], left.at[i]
        )
        out.start()
        sent.append(out)
    for out in sent:
        out.wait()


def pack(up, down, first):
    shape = (up.shape[0], 2 * up.shape[1] - 3 * first)
    return pl.pallas_call(
        functools.partial(pack_body, first),
        in_specs=[pl.BlockSpec(memory_space=pltpu.HBM)] * 2,
        out_specs=pl.BlockSpec(memory_space=pltpu.HBM),
        out_shape=jax.ShapeDtypeStruct(shape, up.dtype),
        scratch_shapes=[
            pltpu.VMEM(shape, up.dtype),
            pltpu.SemaphoreType.DMA((3,)),
            pltpu.SemaphoreType.DMA((3,)),
        ],
        compiler_params=pltpu.CompilerParams(vmem_limit_bytes=62 * 2**20),
        name="pack",
    )(up, down)


def share_of_sum(part, axis):
    peers = lax.axis_size(axis)
    blocks = part.reshape(peers, part.shape[0] // peers, part.shape[1])
    arrived = lax.all_to_all(blocks, axis, split_axis=0, concat_axis=0, tiled=True)
    return arrived.astype(F32).sum(axis=0)


def local(
    tokens,
    pre_attention_gain,
    query_weight,
    key_weight,
    value_weight,
    output_gate_weight,
    decay_weight,
    decay_logit_bias,
    extra_log_decay,
    head_norm_gain,
    attention_out_weight,
    post_attention_gain,
    pre_feedforward_gain,
    post_feedforward_gain,
    up_weight,
    down_weight,
):
    apart = up_weight.shape[1] // 8
    down_rows = down_weight.T
    both = lax.all_gather(pack(up_weight, down_rows, apart), "fs", axis=0, tiled=True)
    groups = lax.axis_size("grp")
    side = lax.rem(lax.axis_index("grp"), 2)
    first = side == 0
    projections = jnp.concatenate(
        [value_weight, output_gate_weight, query_weight, key_weight, decay_weight], 1
    )
    parts = (up_weight[:, : 2 * apart], down_rows[:, :apart], projections, attention_out_weight.T)
    sizes = [p.shape[1] // 2 for p in parts]
    halves = [p[:, h * n : (h + 1) * n] for h in range(2) for p, n in zip(parts, sizes)]
    half = lax.dynamic_slice_in_dim(
        jnp.concatenate(halves, 1), side * sum(sizes), sum(sizes), 1
    )
    sent = (half.astype(F32) * WEIGHT_SCALE).astype(jnp.float16)
    swap = lambda w: lax.ppermute(w, "grp", [(i, i ^ 1) for i in range(groups)])
    far_tokens = swap(tokens)
    held = lax.all_gather(sent, "fs", axis=0, tiled=True)
    far_tokens, held = lax.optimization_barrier((far_tokens, held))
    unscaled = lambda w, lo, hi: (w[:, lo:hi].astype(F32) * (1.0 / WEIGHT_SCALE)).astype(BF16)
    normed = lambda rows: root_norm(rows.astype(F32), pre_attention_gain).astype(BF16)
    edges = [sum(sizes[:i]) for i in range(5)]
    sent_home = jnp.dot(
        normed(far_tokens), unscaled(held, edges[2], edges[3]), preferred_element_type=F32
    )
    acc_far = swap(sent_home)
    tokens, held, sent_home = lax.optimization_barrier((tokens, held, sent_home))
    share = tokens.shape[0] // lax.axis_size("tp")
    own_tokens = lax.dynamic_slice_in_dim(tokens, lax.axis_index("tp") * share, share, 0)
    own_tokens = lax.optimization_barrier(own_tokens.astype(F32))
    acc_near = jnp.dot(
        normed(tokens), unscaled(held, edges[2], edges[3]), preferred_element_type=F32
    )
    dense = lambda w: with_layout_constraint(w, Layout(major_to_minor=(0, 1)))
    near = dense(dense(unscaled(held, edges[3], edges[4])).T)
    far = dense(swap(near))
    acc = jnp.concatenate(
        [jnp.where(first, acc_near, acc_far), jnp.where(first, acc_far, acc_near)], 1
    )
    headout = attend(acc, decay_logit_bias[None], extra_log_decay.T, head_norm_gain[None])

    low, high = headout[:, : sizes[3]], headout[:, sizes[3] :]
    mix_part = sum(
        jnp.dot(h, w, preferred_element_type=F32)
        for h, w in ((jnp.where(first, low, high), near), (jnp.where(first, high, low), far))
    )
    mix_part, held = lax.optimization_barrier((mix_part.astype(BF16), held))
    mixed = share_of_sum(mix_part, "tp")
    apart_near = unscaled(held, 0, edges[2])
    apart_far = swap(apart_near)
    up_apart, down_apart = (
        jnp.concatenate([w[:, lo:hi] for w in (apart_near, apart_far)], 1)
        for lo, hi in zip(edges[:2], edges[1:3])
    )
    stream = own_tokens + root_norm(mixed, post_attention_gain)
    normed_mid = root_norm(stream, pre_feedforward_gain).astype(BF16)
    rows = lax.all_gather(normed_mid, "tp", axis=0, tiled=True)
    act = jnp.square(jax.nn.relu(jnp.dot(rows, up_apart, preferred_element_type=F32))).astype(BF16)
    own, other = act[:, :apart], act[:, apart:]
    early = jnp.where(first, other, own)
    act = jnp.where(first, own, other)
    act = jnp.where(first, act, jnp.roll(act, sizes[1], 1))
    part = lax.dot_general(act, down_apart, (((1,), (1,)), ((), ())), preferred_element_type=F32)
    feed_share = share_of_sum(feed(rows, both, early, part), "tp")
    out_share = (stream + root_norm(feed_share, post_feedforward_gain)).astype(BF16)
    return lax.all_gather(out_share, "tp", axis=0, tiled=True)


def solution(mesh):
    return jax.shard_map(
        local,
        mesh=mesh,
        in_specs=(
            P(("grp", "fs"), None),
            P(),
            P("fs", "tp"),
            P("fs", "tp"),
            P("fs", "tp"),
            P("fs", "tp"),
            P("fs", "tp"),
            P("tp"),
            P(("grp", "fs"), "tp"),
            P("tp"),
            P("tp", "fs"),
            P(),
            P(),
            P(),
            P("fs", "tp"),
            P("tp", "fs"),
        ),
        out_specs=P(("grp", "fs"), None),
        check_vma=False,
    )
```

```python
import functools

import jax
import jax.numpy as jnp
from jax import lax
from jax.experimental import pallas as pl
from jax.experimental.layout import Layout, with_layout_constraint
from jax.experimental.pallas import tpu as pltpu
from jax.sharding import PartitionSpec as P


DK = 64
DV = 128
SUB = 8

EPS = 1e-06
GATE_NORM_SCALE = 16.0
WEIGHT_SCALE = 2.0**16
HIGH = lax.Precision.HIGHEST
F32 = jnp.float32
BF16 = jnp.bfloat16


def root_norm(rows, gain):
    return rows * lax.rsqrt(jnp.mean(rows * rows, axis=-1, keepdims=True) + EPS) * gain


def attend_body(acc_ref, bias_ref, extra_ref, gain_ref, out_ref):
    length = acc_ref.shape[0]
    subs = length // SUB
    rounded = lambda lo, hi: acc_ref[:, lo:hi].astype(BF16).astype(F32)
    v = rounded(0, DV)
    g = rounded(DV, 2 * DV)
    q = rounded(2 * DV, 2 * DV + DK) * DK ** (-0.5)
    k = rounded(2 * DV + DK, 2 * DV + 2 * DK)
    pre = acc_ref[:, 2 * DV + 2 * DK : 2 * DV + 3 * DK] + bias_ref[...]
    log_sig = jnp.minimum(pre, 0.0) - jnp.log1p(jnp.exp(-jnp.abs(pre)))
    log_decay = log_sig / GATE_NORM_SCALE + extra_ref[...].T
    row = lax.broadcasted_iota(jnp.int32, (length, length), 0)
    col = lax.broadcasted_iota(jnp.int32, (length, length), 1)
    dot = functools.partial(lax.dot_general, precision=HIGH, preferred_element_type=F32)
    nn, nt = (((1,), (0,)), ((), ())), (((1,), (1,)), ((), ()))
    cum = dot((row >= col).astype(F32), log_decay, nn)
    cum3, q3, k3 = (a.reshape(subs, SUB, DK) for a in (cum, q, k))
    inside = []
    for j in range(SUB):
        gap = jnp.minimum(cum3 - cum3[:, j : j + 1, :], 0.0)
        inside.append(jnp.sum(q3 * k3[:, j : j + 1, :] * jnp.exp(gap), axis=-1, keepdims=True))
    near = jnp.zeros((length, length), F32)
    for j in range(SUB):
        near = jnp.where(lax.rem(col, SUB) == j, inside[j].reshape(length, 1), near)
    same = (row // SUB == col // SUB) & (row >= col)
    far = [jnp.zeros((SUB, length), F32)]
    for i in range(1, subs):
        at = i * SUB
        mark = cum[at - 1 : at, :]
        left = q[at : at + SUB, :] * jnp.exp(jnp.minimum(cum[at : at + SUB, :] - mark, 0.0))
        right = k * jnp.exp(jnp.minimum(mark - cum, 0.0))
        far.append(dot(left, right, nt))
    scores = jnp.where(same, near, jnp.where(row // SUB > col // SUB, jnp.concatenate(far, 0), 0.0))
    attended = dot(scores, v, nn)
    scaled = attended * lax.rsqrt(jnp.mean(attended * attended, axis=-1, keepdims=True) + EPS)
    out_ref[...] = (scaled * gain_ref[...] * (g / (1.0 + jnp.exp(-g)))).astype(out_ref.dtype)


def attend(acc, bias, extra, gain):
    length = acc.shape[0]
    return pl.pallas_call(
        attend_body,
        out_shape=jax.ShapeDtypeStruct((length, DV), BF16),
        compiler_params=pltpu.CompilerParams(vmem_limit_bytes=16 * 2**20),
        cost_estimate=pl.CostEstimate(flops=40_000_000, bytes_accessed=500_000, transcendentals=400_000),
        name="attend",
    )(acc, bias, extra, gain)


def feed_body(
    halves, rows_ref, weight_ref, last_ref, early_ref, part_ref, out_ref, sum_ref, act_ref
):
    step = pl.program_id(0)

    @pl.when(step < halves)
    def _():
        product = jnp.dot(rows_ref[...], weight_ref[...], preferred_element_type=F32)

        @pl.when(step == 0)
        def _():
            sum_ref[...] = product

        @pl.when(step > 0)
        def _():
            sum_ref[...] += product

        @pl.when(step == halves - 1)
        def _():
            act_ref[...] = jnp.square(jnp.maximum(sum_ref[...], 0.0)).astype(BF16)

    @pl.when(step >= halves)
    def _():
        product = lax.dot_general(
            act_ref[...], weight_ref[...], (((1,), (1,)), ((), ())), preferred_element_type=F32
        )
        product += lax.dot_general(
            early_ref[...], last_ref[...], (((1,), (1,)), ((), ())), preferred_element_type=F32
        )
        out_ref[...] = (product + part_ref[...]).astype(out_ref.dtype)


def feed(rows, both, early, part):
    length, width = rows.shape
    count = early.shape[1]
    units = (both.shape[1] - count) // 2
    halves = 2
    block = width // halves
    later = lambda s: (0, jnp.maximum(s - halves, 0))
    return pl.pallas_call(
        functools.partial(feed_body, halves),
        grid=(2 * halves,),
        in_specs=[
            pl.BlockSpec((length, block), lambda s: (0, jnp.minimum(s, halves - 1))),
            pl.BlockSpec((block, units), lambda s: (lax.rem(s, halves), s // halves)),
            pl.BlockSpec(
                (block, count), lambda s: (jnp.maximum(s - halves, 0), 2 * units // count)
            ),
            pl.BlockSpec((length, count), lambda s: (0, 0)),
            pl.BlockSpec((length, block), later),
        ],
        out_specs=pl.BlockSpec((length, block), later),
        out_shape=jax.ShapeDtypeStruct((length, width), BF16),
        scratch_shapes=[pltpu.VMEM((length, units), F32), pltpu.VMEM((length, units), BF16)],
        compiler_params=pltpu.CompilerParams(
            dimension_semantics=("arbitrary",), vmem_limit_bytes=48 * 2**20
        ),
        cost_estimate=pl.CostEstimate(
            flops=4 * length * width * units, bytes_accessed=4 * width * units, transcendentals=0
        ),
        name="feed",
    )(rows, both, both, early, part)


def pack_body(first, up_ref, down_ref, out_ref, held, arrived, left):
    most = up_ref.shape[1] - 2 * first
    plan = (
        (up_ref, 2 * first, most, 0),
        (down_ref, 2 * first, most, most),
        (down_ref, first, first, 2 * most),
    )
    brought = []
    for i, (source, at, width, to) in enumerate(plan):
        copy = pltpu.make_async_copy(
            source.at[:, pl.ds(at, width)], held.at[:, pl.ds(to, width)], arrived.at[i]
        )
        copy.start()
        brought.append(copy)
    sent = []
    for i, (source, at, width, to) in enumerate(plan):
        brought[i].wait()
        out = pltpu.make_async_copy(
            held.at[:, pl.ds(to, width)], out_ref.at[:, pl.ds(to, width)], left.at[i]
        )
        out.start()
        sent.append(out)
    for out in sent:
        out.wait()


def pack(up, down, first):
    shape = (up.shape[0], 2 * up.shape[1] - 3 * first)
    return pl.pallas_call(
        functools.partial(pack_body, first),
        in_specs=[pl.BlockSpec(memory_space=pltpu.HBM)] * 2,
        out_specs=pl.BlockSpec(memory_space=pltpu.HBM),
        out_shape=jax.ShapeDtypeStruct(shape, up.dtype),
        scratch_shapes=[
            pltpu.VMEM(shape, up.dtype),
            pltpu.SemaphoreType.DMA((3,)),
            pltpu.SemaphoreType.DMA((3,)),
        ],
        compiler_params=pltpu.CompilerParams(vmem_limit_bytes=62 * 2**20),
        name="pack",
    )(up, down)


def share_of_sum(part, axis):
    peers = lax.axis_size(axis)
    blocks = part.reshape(peers, part.shape[0] // peers, part.shape[1])
    arrived = lax.all_to_all(blocks, axis, split_axis=0, concat_axis=0, tiled=True)
    return arrived.astype(F32).sum(axis=0)


def local(
    tokens,
    pre_attention_gain,
    query_weight,
    key_weight,
    value_weight,
    output_gate_weight,
    decay_weight,
    decay_logit_bias,
    extra_log_decay,
    head_norm_gain,
    attention_out_weight,
    post_attention_gain,
    pre_feedforward_gain,
    post_feedforward_gain,
    up_weight,
    down_weight,
):
    apart = up_weight.shape[1] // 8
    down_rows = down_weight.T
    both = lax.all_gather(pack(up_weight, down_rows, apart), "fs", axis=0, tiled=True)
    groups = lax.axis_size("grp")
    side = lax.rem(lax.axis_index("grp"), 2)
    first = side == 0
    projections = jnp.concatenate(
        [value_weight, output_gate_weight, query_weight, key_weight, decay_weight], 1
    )
    parts = (up_weight[:, : 2 * apart], down_rows[:, :apart], projections, attention_out_weight.T)
    sizes = [p.shape[1] // 2 for p in parts]
    halves = [p[:, h * n : (h + 1) * n] for h in range(2) for p, n in zip(parts, sizes)]
    half = lax.dynamic_slice_in_dim(
        jnp.concatenate(halves, 1), side * sum(sizes), sum(sizes), 1
    )
    sent = (half.astype(F32) * WEIGHT_SCALE).astype(jnp.float16)
    swap = lambda w: lax.ppermute(w, "grp", [(i, i ^ 1) for i in range(groups)])
    far_tokens = swap(tokens)
    held = lax.all_gather(sent, "fs", axis=0, tiled=True)
    far_tokens, held = lax.optimization_barrier((far_tokens, held))
    unscaled = lambda w, lo, hi: (w[:, lo:hi].astype(F32) * (1.0 / WEIGHT_SCALE)).astype(BF16)
    normed = lambda rows: root_norm(rows.astype(F32), pre_attention_gain).astype(BF16)
    edges = [sum(sizes[:i]) for i in range(5)]
    sent_home = jnp.dot(
        normed(far_tokens), unscaled(held, edges[2], edges[3]), preferred_element_type=F32
    )
    acc_far = swap(sent_home)
    tokens, held, sent_home = lax.optimization_barrier((tokens, held, sent_home))
    share = tokens.shape[0] // lax.axis_size("tp")
    own_tokens = lax.dynamic_slice_in_dim(tokens, lax.axis_index("tp") * share, share, 0)
    own_tokens = lax.optimization_barrier(own_tokens.astype(F32))
    acc_near = jnp.dot(
        normed(tokens), unscaled(held, edges[2], edges[3]), preferred_element_type=F32
    )
    dense = lambda w: with_layout_constraint(w, Layout(major_to_minor=(0, 1)))
    near = dense(dense(unscaled(held, edges[3], edges[4])).T)
    far = dense(swap(near))
    acc = jnp.concatenate(
        [jnp.where(first, acc_near, acc_far), jnp.where(first, acc_far, acc_near)], 1
    )
    headout = attend(acc, decay_logit_bias[None], extra_log_decay.T, head_norm_gain[None])

    low, high = headout[:, : sizes[3]], headout[:, sizes[3] :]
    mix_part = sum(
        jnp.dot(h, w, preferred_element_type=F32)
        for h, w in ((jnp.where(first, low, high), near), (jnp.where(first, high, low), far))
    )
    mix_part, held = lax.optimization_barrier((mix_part.astype(BF16), held))
    mixed = share_of_sum(mix_part, "tp")
    up_apart, down_apart = [], []
    for side_by_side, lo, hi in ((up_apart, 0, edges[1]), (down_apart, edges[1], edges[2])):
        w = unscaled(held, lo, hi)
        side_by_side += [w, swap(w)]
    up_apart, down_apart = (jnp.concatenate(w, 1) for w in (up_apart, down_apart))
    stream = own_tokens + root_norm(mixed, post_attention_gain)
    normed_mid = root_norm(stream, pre_feedforward_gain).astype(BF16)
    rows = lax.all_gather(normed_mid, "tp", axis=0, tiled=True)
    act = jnp.square(jax.nn.relu(jnp.dot(rows, up_apart, preferred_element_type=F32))).astype(BF16)
    own, other = act[:, :apart], act[:, apart:]
    early = jnp.where(first, other, own)
    act = jnp.where(first, own, other)
    act = jnp.where(first, act, jnp.roll(act, sizes[1], 1))
    part = lax.dot_general(act, down_apart, (((1,), (1,)), ((), ())), preferred_element_type=F32)
    feed_share = share_of_sum(feed(rows, both, early, part), "tp")
    out_share = (stream + root_norm(feed_share, post_feedforward_gain)).astype(BF16)
    return lax.all_gather(out_share, "tp", axis=0, tiled=True)


def solution(mesh):
    return jax.shard_map(
        local,
        mesh=mesh,
        in_specs=(
            P(("grp", "fs"), None),
            P(),
            P("fs", "tp"),
            P("fs", "tp"),
            P("fs", "tp"),
            P("fs", "tp"),
            P("fs", "tp"),
            P("tp"),
            P(("grp", "fs"), "tp"),
            P("tp"),
            P("tp", "fs"),
            P(),
            P(),
            P(),
            P("fs", "tp"),
            P("tp", "fs"),
        ),
        out_specs=P(("grp", "fs"), None),
        check_vma=False,
    )
```
